512 devices in a mesh: ep: 32 (over z, core), tp: 16 (over y, x).
Axes of the slice: x: 4, y: 4, z: 16, core: 2. Of those that a mesh axis runs over, the one named last changes fastest.
Arguments:
- mix_rows: bfloat16 [8192, 2048], P('ep', 'tp'), may hold values from -6 to 6
- mix_gain: bfloat16 [2048], replicated, may hold values from 0.099609375 to 1.8984375
- w_query: bfloat16 [2048, 2048], P(None, 'tp'), may hold values from -0.125 to 0.125
- w_forget: bfloat16 [2048, 2048], P(None, 'tp'), may hold values from -0.125 to 0.125
- w_input: bfloat16 [2048, 2048], P(None, 'tp'), may hold values from -0.125 to 0.125
- w_outgate: bfloat16 [2048, 2048], P(None, 'tp'), may hold values from -0.125 to 0.125
- forget_gap: float32 [2048], P('tp'), may hold values from 1e-05 to 0.1
- decay_extra: float32 [16, 8192], P('tp', 'ep'), may hold values from -0.7 to 0, as said below
- head_gain: bfloat16 [128], replicated, may hold values from 0.099609375 to 1.8984375
- w_mixout: bfloat16 [2048, 2048], P('tp'), may hold values from -0.125 to 0.125
- moe_rows: bfloat16 [8192, 2048], P('ep', 'tp'), may hold values from -6 to 6
- moe_gain: bfloat16 [2048], replicated, may hold values from 0.099609375 to 1.8984375
- route_ids: int32 [8192, 2], P('ep'), may hold values from 0 to 31, all different within a row; in each aligned block of 256 rows (0 to 255, 256 to 511, ...) at most 24 rows name the same one
- route_scores: float32 [8192, 2], P('ep'), may hold values from 0.05 to 1
- w_gate: bfloat16 [32, 2048, 3072], P('ep', None, 'tp'), may hold values from -0.125 to 0.125
- w_up: bfloat16 [32, 2048, 3072], P('ep', None, 'tp'), may hold values from -0.125 to 0.125
- w_down: bfloat16 [32, 3072, 2048], P('ep', 'tp'), may hold values from -0.109375 to 0.109375
Outputs:
- mix_out: bfloat16 [8192, 2048], P('ep', 'tp')
- moe_out: bfloat16 [8192, 2048], P('ep', 'tp')
The draws below stay inside these ranges and needn't reach their ends.
Inputs may be any that keep to these rules, and one draw needn't show every extreme that they name: `route_ids`: each row names 2 different experts. Among the rows of one index of ep at most 24 name the same expert, a bound that at least one block reaches. `decay_extra`: never positive.
All inputs are finite; a program needn't handle non-finite values.
Results may differ from the reference program's by a relative error of at most 0.017.
Values may be sent and summed in bfloat16 or wider, within the bound.
A program may use at most 64 MiB of HBM per device.

```python
import math
import jax
import jax.numpy as jnp
import numpy as np
from jax import lax

HEADS = 16
HEAD_DIM = 128
D = 2048
FFE = 3072
EXPERTS = 32
TOP_K = 2
BLOCK = 64
TOK_A = 256
TOK_B = 256
TOKENS_A = 8192
TOKENS_B = 8192
CAP = 24
N_EP = 32
N_TP = 16


def draw_forget_gap(key, part):
    lowest, highest = (1e-05, 0.1)
    unit = jax.random.uniform(key, (D,), jnp.float32)
    return jnp.exp(jnp.log(lowest) + unit * (jnp.log(highest) - jnp.log(lowest)))


def draw_decay_extra(key, part):
    rate_key, spot_key, depth_key = jax.random.split(key, 3)
    lowest, highest = (1e-05, 0.0001)
    block_list = TOKENS_A // TOK_A
    unit = jax.random.uniform(rate_key, (HEADS, block_list, 1), jnp.float32)
    rate = jnp.exp(jnp.log(lowest) + unit * (jnp.log(highest) - jnp.log(lowest)))
    steady = jnp.broadcast_to(-rate, (HEADS, block_list, TOK_A)).reshape(HEADS, TOKENS_A)
    spots = jax.random.randint(spot_key, (3,), 0, TOKENS_A)
    marked = jnp.any(jnp.arange(TOKENS_A)[None, :] == spots[:, None], axis=0)
    depth = jnp.log(jax.random.uniform(depth_key, (HEADS, TOKENS_A), jnp.float32, 0.5, 0.8))
    return steady + jnp.where(marked[None, :], depth, 0.0)


def block_scale(rng, extent, cuts, smallest, largest):
    factor_of = 1.0
    for position, shards_of in cuts:
        draws = jax.random.uniform(jax.random.fold_in(jax.random.fold_in(rng, 6), position), (shards_of,), jnp.float32, smallest / len(cuts), largest / len(cuts))
        factor_of = factor_of * jnp.repeat(jnp.exp(draws), extent[position] // shards_of).reshape((-1,) + (1,) * (len(extent) - 1 - position))
    return factor_of


def assign_block(key, own, number, rows, amount, top, limit, skew):
    ranking = jax.random.permutation(key, amount)
    crowded, common = load_shares(amount, rows * top, limit, skew, True), load_shares(amount, rows * top, limit, skew, False)
    places = jnp.arange(amount)

    def named(tallies, offset_by):
        used = int((tallies > 0).sum())
        fixed = max(1, used // 4)
        moved = fixed + (places - fixed + offset_by * (used - fixed)) % max(1, amount - fixed)
        return jnp.zeros((amount,), jnp.int32).at[ranking[jnp.where(places < fixed, places, moved)]].set(jnp.asarray(tallies, jnp.int32))

    tallies = jnp.where(number % 4 == 0, named(crowded, number // 4), named(common, number - number // 4 - 1))
    mixed = jax.random.permutation(jax.random.fold_in(own, 3), amount)
    source_of, taker = mixed[0:amount // 2 * 2:2], mixed[1:amount // 2 * 2:2]
    margin = jnp.minimum(tallies[source_of] - 1, limit - tallies[taker]) // 2
    margin = jnp.where((source_of == ranking[0]) | (taker == ranking[0]) | (tallies[taker] == 0), 0, jnp.maximum(margin, 0))
    moved = jax.random.randint(jax.random.fold_in(own, 4), (amount // 2,), 0, 1 << 20) % (margin + 1)
    tallies = tallies.at[source_of].add(-moved).at[taker].add(moved)
    members = jnp.searchsorted(jnp.cumsum(tallies), jnp.arange(rows * top), side="right").astype(jnp.int32)
    table = members.reshape(top, rows).T
    table = table[jax.random.permutation(jax.random.fold_in(own, 1), rows)]
    offset_by = jax.random.randint(jax.random.fold_in(own, 2), (rows, 1), 0, top)
    return jnp.take_along_axis(table, (jnp.arange(top)[None, :] + offset_by) % top, axis=1)


def load_shares(count, total, limit, skew, full):
    portions = [(1 << 20) // math.isqrt(standing ** skew) + 1 for standing in range(1, count + 1)]
    largest = limit if full else min(limit, max(-(-total // count), total * portions[0] // sum(portions)))
    least = 1 if total - largest >= count - 1 else 0
    counts, surplus = [largest] + [least] * (count - 1), total - largest - least * (count - 1)
    while surplus > 0:
        candidates = [i for i in range(1, count) if counts[i] < largest] or [i for i in range(1, count) if counts[i] < limit]
        mass, remaining = sum([portions[i] for i in candidates]), surplus
        for i in candidates:
            addition = min(limit - counts[i], max(1, remaining * portions[i] // mass), surplus)
            counts[i] = counts[i] + addition
            surplus = surplus - addition
    return np.array(counts)


def bell_draw(stream_key, extent, scale, bound, shards=(), held_as=jnp.bfloat16):
    loudness = block_scale(stream_key, extent, shards, -0.22, 0.18) if shards else 1.0
    drawn = jax.random.normal(stream_key, extent, jnp.float32) * scale * loudness
    return jnp.minimum(jnp.maximum(drawn, -bound), bound).astype(held_as)


def setup_inputs(seed: int = 0) -> dict:
    splits = jax.random.split(jax.random.key(seed), 18)
    mix_rows = bell_draw(splits[0], (TOKENS_A, D), 1.0, 6.0, ((0, 32), (1, 16)))
    mix_gain = jnp.clip(1.0 + 0.18 * jax.random.normal(splits[1], (D,), jnp.float32), 0.099609375, 1.8984375).astype(jnp.bfloat16)
    w_query = bell_draw(splits[2], (D, D), D ** -0.5, 0.125, ((1, 16),))
    w_forget = bell_draw(splits[3], (D, D), D ** -0.5, 0.125, ((1, 16),))
    w_input = bell_draw(splits[4], (D, D), D ** -0.5, 0.125, ((1, 16),))
    w_outgate = bell_draw(splits[5], (D, D), D ** -0.5, 0.125, ((1, 16),))
    forget_gap = draw_forget_gap(jax.random.fold_in(splits[17], 71), 0)
    decay_extra = draw_decay_extra(jax.random.fold_in(splits[17], 71), 0)
    head_gain = jnp.clip(1.0 + 0.18 * jax.random.normal(splits[8], (HEAD_DIM,), jnp.float32), 0.099609375, 1.8984375).astype(jnp.bfloat16)
    w_mixout = bell_draw(splits[9], (D, D), D ** -0.5, 0.125, ((0, 16),))
    moe_rows = bell_draw(splits[10], (TOKENS_B, D), 1.0, 6.0, ((0, 32), (1, 16)))
    moe_gain = jnp.clip(1.0 + 0.18 * jax.random.normal(splits[11], (D,), jnp.float32), 0.099609375, 1.8984375).astype(jnp.bfloat16)
    route_ids_keys = jax.random.split(jax.random.fold_in(splits[12], 1), TOKENS_B // TOK_B)
    route_ids_turns = jax.random.permutation(jax.random.fold_in(splits[12], 3), TOKENS_B // TOK_B)
    route_ids = jax.vmap(lambda own, number: assign_block(jax.random.fold_in(splits[12], 2), own, number, TOK_B, EXPERTS, TOP_K, CAP, 1))(route_ids_keys, route_ids_turns).reshape((TOKENS_B, TOP_K))
    route_scores = jnp.clip(0.05 + 0.95 * jax.random.uniform(splits[13], (TOKENS_B, TOP_K), jnp.float32) ** block_scale(splits[13], (TOKENS_B, TOP_K), ((0, 32),), -0.2, 0.2), 0.05, 1.0)
    w_gate = bell_draw(splits[14], (EXPERTS, D, FFE), D ** -0.5, 0.125, ((0, 32), (2, 16)))
    w_up = bell_draw(splits[15], (EXPERTS, D, FFE), D ** -0.5, 0.125, ((0, 32), (2, 16)))
    w_down = bell_draw(splits[16], (EXPERTS, FFE, D), FFE ** -0.5, 0.109375, ((0, 32), (1, 16)))
    return dict(mix_rows=mix_rows, mix_gain=mix_gain, w_query=w_query, w_forget=w_forget, w_input=w_input, w_outgate=w_outgate, forget_gap=forget_gap, decay_extra=decay_extra, head_gain=head_gain, w_mixout=w_mixout, moe_rows=moe_rows, moe_gain=moe_gain, route_ids=route_ids, route_scores=route_scores, w_gate=w_gate, w_up=w_up, w_down=w_down)


epsilon = 1e-06
HIGHEST_PRECISION = lax.Precision.HIGHEST

def rms_scale(rows, gain):
    values = rows.astype(jnp.float32)
    scale = lax.rsqrt(lax.optimization_barrier(jnp.mean(values * values, axis=-1, keepdims=True)) + epsilon)
    return values * scale * gain.astype(jnp.float32)

def block_recurrence(query_rows, key_in, value, log_forget, state):
    heads_count, length, key_dim = query_rows.shape
    block_list = length // BLOCK

    def split(values):
        return jnp.moveaxis(values.reshape(heads_count, block_list, BLOCK, values.shape[2]), 1, 0)
    causal = jnp.tril(jnp.ones((BLOCK, BLOCK), dtype=bool))[:, :, None]

    def advance(carry, inputs):
        query_block, key_block, value_block, forget_block = inputs
        running_state = jnp.cumsum(forget_block, axis=1)
        spread = running_state[:, :, None, :] - running_state[:, None, :, :]
        decay = jnp.exp(jnp.where(causal, spread, -jnp.inf))
        scores = jnp.einsum('hid,hjd,hijd->hij', query_block, key_block, decay, precision=HIGHEST_PRECISION)
        output = jnp.einsum('hid,hde->hie', query_block * jnp.exp(running_state), carry, precision=HIGHEST_PRECISION)
        output = output + jnp.einsum('hij,hje->hie', scores, value_block, precision=HIGHEST_PRECISION)
        last = running_state[:, -1:, :]
        carry = carry * jnp.exp(last)[:, 0, :, None] + jnp.einsum('hjd,hje->hde', key_block * jnp.exp(last - running_state), value_block, precision=HIGHEST_PRECISION)
        return (carry, output)
    carry, outputs = lax.scan(advance, state, (split(query_rows), split(key_in), split(value), split(log_forget)))
    return (jnp.moveaxis(outputs, 0, 1).reshape(heads_count, length, value.shape[2]), carry)

def token_mixer(mix_rows, mix_gain, w_query, w_forget, w_input, w_outgate, forget_gap, decay_extra, head_gain, w_mixout):
    normed = rms_scale(mix_rows, mix_gain).astype(jnp.bfloat16)
    length = normed.shape[0]
    query_preactivation = jnp.dot(normed, w_query, preferred_element_type=jnp.float32)
    forget_pre = jnp.dot(normed, w_forget, preferred_element_type=jnp.float32)
    input_pre = jnp.dot(normed, w_input, preferred_element_type=jnp.float32)
    outgate_pre = jnp.dot(normed, w_outgate, preferred_element_type=jnp.float32)

    def heads(values):
        return values.reshape(length, HEADS, HEAD_DIM).transpose(1, 0, 2)
    query_rows = heads(jax.nn.silu(query_preactivation))
    key_in = heads(forget_gap.astype(jnp.float32) * jax.nn.sigmoid(-forget_pre))
    value = heads(input_pre)
    log_forget = jnp.log1p(-key_in) + decay_extra.astype(jnp.float32)[:, :, None]
    start_state = jnp.zeros((HEADS, HEAD_DIM, HEAD_DIM), jnp.float32)
    head_out, _ = block_recurrence(query_rows, key_in, value, log_forget, start_state)
    gated = rms_scale(head_out, head_gain) * heads(jax.nn.silu(outgate_pre))
    gated = gated.transpose(1, 0, 2).reshape(length, D).astype(jnp.bfloat16)
    group = D // N_TP
    total = jnp.zeros((length, D), jnp.float32)
    for index in range(N_TP):
        part = jnp.dot(gated[:, index * group:(index + 1) * group], w_mixout[index * group:(index + 1) * group], preferred_element_type=jnp.float32)
        total = total + lax.optimization_barrier(part.astype(jnp.bfloat16)).astype(jnp.float32)
    return total.astype(jnp.bfloat16)

def expert_layer(moe_rows, moe_gain, route_ids, route_scores, w_gate, w_up, w_down):
    row_total, top_count = route_ids.shape
    expert_count = w_gate.shape[0]
    normed = rms_scale(moe_rows, moe_gain).astype(jnp.bfloat16)
    weights = route_scores / lax.optimization_barrier(jnp.sum(route_scores, axis=1, keepdims=True))
    grouped = route_ids.reshape(N_EP, TOK_B * top_count).astype(jnp.int32)
    onehot = (grouped[:, :, None] == jnp.arange(expert_count, dtype=jnp.int32)[None, None, :]).astype(jnp.int32)
    rank = lax.optimization_barrier(jnp.sum((jnp.cumsum(onehot, axis=1) - 1) * onehot, axis=2)).astype(jnp.int32)
    source = jnp.arange(N_EP, dtype=jnp.int32)[:, None]
    place = (grouped * (N_EP * CAP) + source * CAP + rank).reshape(-1).astype(jnp.int32)
    token = (jnp.arange(row_total * top_count, dtype=jnp.int32) // top_count).astype(jnp.int32)
    table = jnp.full((expert_count * N_EP * CAP,), row_total, jnp.int32).at[place].set(token)
    padded = jnp.concatenate([normed, jnp.zeros((1, D), jnp.bfloat16)], axis=0)
    slots = padded[table].reshape(expert_count, N_EP * CAP, D)
    width = FFE // N_TP

    def one_expert(operands):
        rows, gate_weight, up_weight, down_weight = operands
        gate_acts = jnp.dot(rows, gate_weight, preferred_element_type=jnp.float32)
        up_acts = jnp.dot(rows, up_weight, preferred_element_type=jnp.float32)
        hidden = (jax.nn.silu(gate_acts) * up_acts).astype(jnp.bfloat16)
        total = jnp.zeros((rows.shape[0], D), jnp.float32)
        for index in range(N_TP):
            part = jnp.dot(hidden[:, index * width:(index + 1) * width], down_weight[index * width:(index + 1) * width], preferred_element_type=jnp.float32)
            total = total + lax.optimization_barrier(part.astype(jnp.bfloat16)).astype(jnp.float32)
        return total.astype(jnp.bfloat16)
    results = lax.map(one_expert, (slots, w_gate, w_up, w_down)).reshape(-1, D)
    picked = results[place].astype(jnp.float32).reshape(row_total, top_count, D)
    return lax.optimization_barrier(jnp.sum(picked * weights[:, :, None], axis=1)).astype(jnp.bfloat16)

def reference(mix_rows, mix_gain, w_query, w_forget, w_input, w_outgate, forget_gap, decay_extra, head_gain, w_mixout, moe_rows, moe_gain, route_ids, route_scores, w_gate, w_up, w_down):
    mix_out = token_mixer(mix_rows, mix_gain, w_query, w_forget, w_input, w_outgate, forget_gap, decay_extra, head_gain, w_mixout)
    moe_out = expert_layer(moe_rows, moe_gain, route_ids, route_scores, w_gate, w_up, w_down)
    return (mix_out, moe_out)
```

```python
import functools

import jax
import jax.numpy as jnp
from jax import lax
from jax.experimental import pallas as pl
from jax.experimental.pallas import tpu as pltpu
from jax.sharding import PartitionSpec as P

MESH = pl.DeviceIdType.MESH
epsilon = 1e-06
HIGHEST = lax.Precision.HIGHEST
F32, BF16 = jnp.float32, jnp.bfloat16
SIDE = 4
COL = 128
GROUP = SIDE * COL


def dot(a, b):
    return jnp.dot(a, b, preferred_element_type=F32)


def dot_t(a, b):
    return lax.dot_general(a, b, (((1,), (1,)), ((), ())), preferred_element_type=F32)


def step_kernel(
    n_ep,
    cap,
    mix_rows,
    moe_rows,
    gains,
    gap,
    decay,
    head_gain,
    ids,
    scores,
    wq_h,
    wf_h,
    wi_h,
    wo_h,
    wmix_h,
    wg_h,
    wu_h,
    wd_h,
    mix_out,
    moe_out,
    wm,
    wmix,
    wg,
    wu,
    wd,
    slots,
    arrived,
    outgoing,
    returned,
    places,
    xa,
    xb,
    ma,
    mb,
    acc_x,
    sq_x,
    acc_g,
    acc_u,
    sq_m,
    st_out,
    st_in,
    st_back,
    st_enter,
    pxa,
    pxb,
    oxa,
    oxb,
    nxa,
    nxb,
    pma,
    pmb,
    oma,
    omb,
    nma,
    nmb,
    o2xa,
    o2xb,
    n2xa,
    n2xb,
    o2ma,
    o2mb,
    n2ma,
    n2mb,
    wsem,
    a2a_s,
    a2a_r,
    agx_s,
    agx_r,
    agm_s,
    agm_r,
    rsx_s,
    rsx_r,
    rsm_s,
    rsm_r,
):
    n_z = n_ep // 2
    ep = lax.axis_index("ep")
    tp = lax.axis_index("tp")
    x, y = lax.rem(tp, SIDE), tp // SIDE
    z, core = ep // 2, lax.rem(ep, 2)

    def on(v, d):
        return lax.rem(v + d + SIDE, SIDE)

    x_plus, x_minus = (ep, y * SIDE + on(x, 1)), (ep, y * SIDE + on(x, -1))
    y_plus, y_minus = (ep, on(y, 1) * SIDE + x), (ep, on(y, -1) * SIDE + x)

    loads = [
        pltpu.make_async_copy(src, dst, wsem.at[i])
        for i, (src, dst) in enumerate(
            [
                (wq_h, wm.at[:, 0:COL]),
                (wf_h, wm.at[:, COL : 2 * COL]),
                (wi_h, wm.at[:, 2 * COL : 3 * COL]),
                (wo_h, wm.at[:, 3 * COL : 4 * COL]),
                (wg_h.at[0], wg),
                (wu_h.at[0], wu),
                (wd_h.at[0], wd),
                (wmix_h, wmix),
            ]
        )
    ]
    for load in loads:
        load.start()

    barrier = pltpu.get_barrier_semaphore()
    for peer in (x_plus, x_minus, y_plus, y_minus):
        pl.semaphore_signal(barrier, inc=1, device_id=peer, device_id_type=MESH)

    def greet(o, carry):
        pl.semaphore_signal(
            barrier, inc=1, device_id=(lax.rem(ep + o, n_ep), tp), device_id_type=MESH
        )
        return carry

    lax.fori_loop(1, n_ep, greet, 0)

    tok = ids.shape[1]
    id0, id1 = ids[0:1], ids[1:2]
    expert = lax.broadcasted_iota(jnp.int32, (n_ep, tok), 0)
    one0, one1 = expert == id0, expert == id1
    named = jnp.where(one0 | one1, 1.0, 0.0).astype(BF16)
    row = lax.broadcasted_iota(jnp.int32, (tok, tok), 0)
    col = lax.broadcasted_iota(jnp.int32, (tok, tok), 1)
    before = jnp.where(row < col, 1.0, 0.0).astype(BF16)
    rank = dot(named, before)
    place0 = id0.astype(F32) * cap + jnp.sum(jnp.where(one0, rank, 0.0), axis=0, keepdims=True)
    place1 = id1.astype(F32) * cap + jnp.sum(jnp.where(one1, rank, 0.0), axis=0, keepdims=True)
    line = lax.broadcasted_iota(jnp.int32, (COL, tok), 0)
    table = jnp.where(line == 0, place0, place1)
    table = jnp.where(line == 2, scores[0:1], jnp.where(line == 3, scores[1:2], table))
    places[...] = table.T
    slot = lax.broadcasted_iota(jnp.int32, (n_ep * cap, tok), 0).astype(F32)
    pick = jnp.where((slot == place0) | (slot == place1), 1.0, 0.0).astype(BF16)
    slots[...] = dot(pick, moe_rows[...]).reshape(n_ep, cap, COL).astype(BF16)

    half_x = xa.shape[1]
    mine_a, mine_b = y * SIDE + x, x * SIDE + y
    xa[mine_a] = mix_rows[0:half_x]
    xb[mine_b] = mix_rows[half_x : 2 * half_x]

    pl.semaphore_wait(barrier, n_ep - 1 + 4)

    def exchange(src, dst, k):
        def send(o, carry):
            peer = lax.rem(ep + o, n_ep)
            pltpu.make_async_remote_copy(
                src_ref=src.at[peer],
                dst_ref=dst.at[ep],
                send_sem=a2a_s.at[k],
                recv_sem=a2a_r.at[k],
                device_id=(peer, tp),
                device_id_type=MESH,
            ).start()
            return carry

        lax.fori_loop(1, n_ep, send, 0)
        dst[ep] = src[ep]

    def whole(src, dst, k, count):
        return pltpu.make_async_remote_copy(
            src_ref=src.at[pl.ds(0, count)],
            dst_ref=dst.at[pl.ds(0, count)],
            send_sem=a2a_s.at[k],
            recv_sem=a2a_r.at[k],
            device_id=(lax.rem(ep + 1, n_ep), tp),
            device_id_type=MESH,
        )

    class Gather:
        def __init__(self, buf, outer, inner, out_plus, out_minus, in_plus, in_minus, s, r):
            self.buf, self.outer, self.inner = buf, outer, inner
            self.op, self.om, self.ip, self.im = out_plus, out_minus, in_plus, in_minus
            self.s, self.r = s, r
            self.h = buf.shape[1]

        def at(self, do, di):
            return on(self.outer, do) * SIDE + on(self.inner, di)

        def copy(self, block, rows, sem, to):
            ref = self.buf.at[block] if rows is None else self.buf.at[block, pl.ds(*rows)]
            return pltpu.make_async_remote_copy(
                src_ref=ref,
                dst_ref=ref,
                send_sem=self.s,
                recv_sem=self.r.at[sem],
                device_id=to,
                device_id_type=MESH,
            )

        def first(self):
            q = self.h // 2
            self.lo, self.hi = (0, q), (q, q)
            self.copy(self.at(0, 0), None, 0, self.ip).start()
            self.copy(self.at(0, 0), None, 1, self.im).start()

        def cross(self, di, sem):
            self.copy(self.at(0, di), None, sem, self.op).start()
            self.copy(self.at(0, di), None, sem + 1, self.om).start()

        def near(self):
            self.copy(self.at(0, -1), None, 0, self.ip).wait_recv()
            self.copy(self.at(0, -1), self.lo, 2, self.ip).start()
            self.copy(self.at(0, 1), None, 1, self.im).wait_recv()
            self.copy(self.at(0, 1), self.hi, 3, self.im).start()

        def far(self):
            self.copy(self.at(0, 2), self.lo, 2, self.ip).wait_recv()
            self.copy(self.at(0, 2), self.hi, 3, self.im).wait_recv()

        def relay(self, di, sem):
            self.copy(self.at(-1, di), None, sem, self.op).wait_recv()
            self.copy(self.at(-1, di), self.lo, sem + 2, self.op).start()
            self.copy(self.at(1, di), None, sem + 1, self.om).wait_recv()
            self.copy(self.at(1, di), self.hi, sem + 3, self.om).start()

        def last(self, di, sem):
            self.copy(self.at(2, di), self.lo, sem + 2, self.op).wait_recv()
            self.copy(self.at(2, di), self.hi, sem + 3, self.om).wait_recv()

        def drain(self):
            ref = self.buf.at[pl.ds(0, SIDE * SIDE - 1)]
            pltpu.make_async_remote_copy(
                src_ref=ref,
                dst_ref=ref,
                send_sem=self.s,
                recv_sem=self.r.at[0],
                device_id=self.op,
                device_id_type=MESH,
            ).wait_send()

    def gathers(a, b, s, r):
        return (
            Gather(a, y, x, y_plus, y_minus, x_plus, x_minus, s.at[0], r.at[0]),
            Gather(b, x, y, x_plus, x_minus, y_plus, y_minus, s.at[1], r.at[1]),
        )

    crossings = ((0, 4), (-1, 8), (1, 12), (2, 16))

    def gather_start(pair):
        for g in pair:
            g.first()
        for g in pair:
            g.cross(0, 4)

    def gather_near(pair):
        for g in pair:
            g.near()
        for g in pair:
            g.cross(-1, 8)
            g.cross(1, 12)

    def gather_far(pair):
        for g in pair:
            g.far()
            g.cross(2, 16)

    def gather_relays(pair):
        for di, sem in crossings:
            for g in pair:
                g.relay(di, sem)

    def gather_last(pair):
        for di, sem in crossings:
            for g in pair:
                g.last(di, sem)

    ones = jnp.ones((GROUP, COL), BF16)

    def features(is_a, group, j):
        return group * SIDE + j if is_a else j * SIDE + group

    def weight_rows(ref, is_a, group):
        if is_a:
            return ref[pl.ds(pl.multiple_of(group * GROUP, GROUP), GROUP), :]
        return jnp.concatenate(
            [
                ref[pl.ds(pl.multiple_of(features(False, group, j) * COL, COL), COL), :]
                for j in range(SIDE)
            ],
            axis=0,
        )

    def weight_columns(ref, is_a, group):
        if is_a:
            return ref[:, pl.ds(pl.multiple_of(group * GROUP, GROUP), GROUP)]
        return jnp.concatenate(
            [
                ref[:, pl.ds(pl.multiple_of(features(False, group, j) * COL, COL), COL)]
                for j in range(SIDE)
            ],
            axis=1,
        )

    def use_rows(buf, is_a, group, gain_at, outs, sq, start):
        h = buf.shape[1]
        scaled, squares = [], []
        for j in range(SIDE):
            part = buf[group * SIDE + j].astype(F32)
            scaled.append((part * gains[gain_at + features(is_a, group, j)]).astype(BF16))
            squares.append((part * part).astype(BF16))
        scaled, squares = jnp.concatenate(scaled, axis=1), jnp.concatenate(squares, axis=1)
        rows = pl.ds(0 if is_a else h, h)
        found = [(sq, dot(squares, ones))]
        for ref, acc in outs:
            if ref.shape[0] > ref.shape[1]:
                found.append((acc, dot(scaled, weight_rows(ref, is_a, group))))
            else:
                found.append((acc, dot_t(scaled, weight_columns(ref, is_a, group))))
        for acc, got in found:
            acc[rows, :] = got if start else acc[rows, :] + got

    class Scatter:
        def __init__(self, p, o1, n1, o2, n2, outer, inner, op, om, ip, im, s, r, make):
            self.p, self.o1, self.n1, self.o2, self.n2 = p, o1, n1, o2, n2
            self.outer, self.inner = outer, inner
            self.op, self.om, self.ip, self.im = op, om, ip, im
            self.s, self.r, self.make = s, r, make
            self.h = p.shape[1]
            self.q = self.h // 2
            self.lo, self.hi = pl.ds(0, self.q), pl.ds(self.q, self.q)

        def copy(self, src, dst, sem, to):
            return pltpu.make_async_remote_copy(
                src_ref=src,
                dst_ref=dst,
                send_sem=self.s,
                recv_sem=self.r.at[sem],
                device_id=to,
                device_id_type=MESH,
            )

        def produce(self, do):
            group = on(self.outer, do)
            got = self.make(group)
            for j in range(SIDE):
                self.p[group * SIDE + j] = got[:, j * COL : (j + 1) * COL].astype(BF16)

        def group(self, do, rows):
            return self.p.at[pl.ds(on(self.outer, do) * SIDE, SIDE), rows]

        def block(self, di, rows):
            return self.p.at[self.outer * SIDE + on(self.inner, di), rows]

        def leg1(self, name):
            return dict(
                a=lambda: self.copy(self.group(2, self.lo), self.o1.at[0], 0, self.op),
                b=lambda: self.copy(self.group(2, self.hi), self.o1.at[1], 1, self.om),
                c=lambda: self.copy(self.group(1, self.hi), self.n1.at[0, :, self.hi], 2, self.op),
                d=lambda: self.copy(self.group(-1, self.lo), self.n1.at[1, :, self.lo], 3, self.om),
                e=lambda: self.copy(self.group(1, self.lo), self.n1.at[0, :, self.lo], 4, self.op),
                f=lambda: self.copy(self.group(-1, self.hi), self.n1.at[1, :, self.hi], 5, self.om),
            )[name]()

        def leg2(self, name):
            return dict(
                a=lambda: self.copy(self.block(2, self.lo), self.o2.at[0], 6, self.ip),
                b=lambda: self.copy(self.block(2, self.hi), self.o2.at[1], 7, self.im),
                c=lambda: self.copy(self.block(1, self.hi), self.n2.at[0, self.hi], 8, self.ip),
                d=lambda: self.copy(self.block(-1, self.lo), self.n2.at[1, self.lo], 9, self.im),
                e=lambda: self.copy(self.block(1, self.lo), self.n2.at[0, self.lo], 10, self.ip),
                f=lambda: self.copy(self.block(-1, self.hi), self.n2.at[1, self.hi], 11, self.im),
            )[name]()

        def start1(self):
            self.produce(2)
            self.leg1("a").start()
            self.leg1("b").start()

        def direct1(self):
            self.produce(1)
            self.leg1("c").start()
            self.produce(-1)
            self.leg1("d").start()

        def add(self, dst, src):
            dst[...] = (dst[...].astype(F32) + src[...].astype(F32)).astype(BF16)

        def relay1(self):
            self.leg1("a").wait_recv()
            self.add(self.group(1, self.lo), self.o1.at[0])
            self.leg1("e").start()
            self.leg1("b").wait_recv()
            self.add(self.group(-1, self.hi), self.o1.at[1])
            self.leg1("f").start()

        def settle1(self):
            for leg in "cdef":
                self.leg1(leg).wait_recv()
            here = self.p.at[pl.ds(self.outer * SIDE, SIDE)]
            here[...] = (
                here[...].astype(F32) + self.n1[0].astype(F32) + self.n1[1].astype(F32)
            ).astype(BF16)
            for leg in "abcd":
                self.leg2(leg).start()

        def relay2(self):
            self.leg2("a").wait_recv()
            self.add(self.block(1, self.lo), self.o2.at[0])
            self.leg2("e").start()
            self.leg2("b").wait_recv()
            self.add(self.block(-1, self.hi), self.o2.at[1])
            self.leg2("f").start()

        def settle2(self):
            for leg in "cdef":
                self.leg2(leg).wait_recv()
            mine = self.p[self.outer * SIDE + self.inner].astype(F32)
            return mine + self.n2[0].astype(F32) + self.n2[1].astype(F32)

        def drain(self):
            ref = self.p.at[pl.ds(0, SIDE * SIDE - 1)]
            self.copy(ref, ref, 0, self.op).wait_send()

    def scatters(left, w, pa, pb, oa, ob, na, nb, o2a, o2b, n2a, n2b, s, r):
        h = pa.shape[1]

        def make_a(group):
            return dot(left()[0:h], weight_columns(w, True, group))

        def make_b(group):
            return dot(left()[h : 2 * h], weight_columns(w, False, group))

        return (
            Scatter(
                pa, oa, na, o2a, n2a, y, x, y_plus, y_minus, x_plus, x_minus, s.at[0], r.at[0], make_a
            ),
            Scatter(
                pb, ob, nb, o2b, n2b, x, y, x_plus, x_minus, y_plus, y_minus, s.at[1], r.at[1], make_b
            ),
        )

    def scatter_all(pair):
        for g in pair:
            g.start1()
        for g in pair:
            g.direct1()
        for g in pair:
            g.relay1()
        for g in pair:
            g.produce(0)
        for g in pair:
            g.settle1()
        for g in pair:
            g.relay2()
        got = [g.settle2() for g in pair]
        for g in pair:
            g.drain()
        return got

    exchange(slots, arrived, 0)
    mix = gathers(xa, xb, agx_s, agx_r)
    gather_start(mix)
    gather_near(mix)
    for load in loads[0:4]:
        load.wait()
    gather_far(mix)
    xo = [(wm, acc_x)]
    use_rows(xa, True, y, 0, xo, sq_x, True)
    use_rows(xb, False, x, 0, xo, sq_x, True)
    gather_relays(mix)
    for d in (-1, 1):
        use_rows(xa, True, on(y, d), 0, xo, sq_x, False)
        use_rows(xb, False, on(x, d), 0, xo, sq_x, False)
    gather_last(mix)
    use_rows(xa, True, on(y, 2), 0, xo, sq_x, False)
    use_rows(xb, False, on(x, 2), 0, xo, sq_x, False)
    for g in mix:
        g.drain()

    width = SIDE * SIDE * COL
    scale = lax.rsqrt(sq_x[...] * (1.0 / width) + epsilon)
    query = jax.nn.silu(acc_x[:, 0:COL] * scale)
    key = gap[...] * jax.nn.sigmoid(-(acc_x[:, COL : 2 * COL] * scale))
    value = (acc_x[:, 2 * COL : 3 * COL] * scale).astype(BF16)
    gate_out = jax.nn.silu(acc_x[:, 3 * COL : 4 * COL] * scale)
    extra = jnp.broadcast_to(decay[...], (COL, decay.shape[1])).T
    log_forget = jnp.log1p(-key) + extra
    part = half_x
    row = lax.broadcasted_iota(jnp.int32, (part, part), 0)
    col = lax.broadcasted_iota(jnp.int32, (part, part), 1)
    causal = row >= col
    lower = jnp.where(causal, 1.0, 0.0)
    outs, running, states, ends = [], [], [], []
    for c in range(2):
        rows = slice(c * part, (c + 1) * part)
        run = jnp.dot(lower, log_forget[rows], precision=HIGHEST, preferred_element_type=F32)
        mid, end = run[part // 2 - 1 : part // 2], run[part - 1 : part]
        q_in = (query[rows] * jnp.exp(run - mid)).astype(BF16)
        k_in = (key[rows] * jnp.exp(mid - run)).astype(BF16)
        near = lax.dot_general(q_in, k_in, (((1,), (1,)), ((), ())), preferred_element_type=F32)
        near = jnp.where(causal, near, 0.0).astype(BF16)
        outs.append(dot(near, value[rows]))
        k_end = (key[rows] * jnp.exp(end - run)).astype(BF16)
        states.append(
            lax.dot_general(value[rows], k_end, (((0,), (0,)), ((), ())), preferred_element_type=F32)
        )
        running.append(run)
        ends.append(end)
    q_second = (query[part:] * jnp.exp(running[1])).astype(BF16)
    outs[1] = outs[1] + lax.dot_general(
        q_second, states[0].astype(BF16), (((1,), (1,)), ((), ())), preferred_element_type=F32
    )
    state = states[0] * jnp.exp(ends[1]) + states[1]
    passing = jnp.exp(ends[0] + ends[1])
    q_enter = jnp.concatenate(
        [
            (query[:part] * jnp.exp(running[0])).astype(BF16),
            (query[part:] * jnp.exp(ends[0] + running[1])).astype(BF16),
        ],
        axis=0,
    )
    local_out = jnp.concatenate(outs, axis=0)
    slices = COL // 8
    st_out[...] = jnp.concatenate(
        [
            state.reshape(slices, 8, COL),
            jnp.broadcast_to(passing.reshape(1, 1, COL), (slices, 8, COL)),
        ],
        axis=1,
    ).astype(BF16)

    owner = core == lax.rem(z, 2)
    not_owner = jnp.logical_not(owner)

    def to_owner(k, carry):
        peer = 2 * k + lax.rem(k, 2)

        @pl.when(peer != ep)
        def _():
            pltpu.make_async_remote_copy(
                src_ref=st_out.at[k],
                dst_ref=st_in.at[ep],
                send_sem=a2a_s.at[2],
                recv_sem=a2a_r.at[2],
                device_id=(peer, tp),
                device_id_type=MESH,
            ).start()

        return carry

    lax.fori_loop(0, slices, to_owner, 0)

    @pl.when(owner)
    def _():
        st_in[ep] = st_out[z]

    whole(slots, arrived, 0, n_ep - 1).wait_recv()
    half_m = ma.shape[1]
    got = arrived[...].astype(F32).reshape(2 * half_m, COL).astype(BF16)
    ma[mine_a] = got[0:half_m]
    mb[mine_b] = got[half_m:]
    moe = gathers(ma, mb, agm_s, agm_r)
    gather_start(moe)
    for load in loads[4:]:
        load.wait()
    mo = [(wg, acc_g), (wu, acc_u)]
    moe_gain_at = SIDE * SIDE
    gather_near(moe)

    @pl.when(owner)
    def _():
        whole(st_in, st_in, 2, n_ep - 1).wait_recv()

        def chain(j, entering):
            block = st_in[j].astype(F32)
            st_back[j] = entering
            return block[8:16] * entering + block[0:8]

        lax.fori_loop(0, n_ep, chain, jnp.zeros((8, COL), F32))

        def give(o, carry):
            peer = lax.rem(ep + o, n_ep)
            pltpu.make_async_remote_copy(
                src_ref=st_back.at[peer],
                dst_ref=st_enter.at[z],
                send_sem=a2a_s.at[3],
                recv_sem=a2a_r.at[3],
                device_id=(peer, tp),
                device_id_type=MESH,
            ).start()
            return carry

        lax.fori_loop(1, n_ep, give, 0)
        st_enter[z] = st_back[ep]

    gather_far(moe)
    use_rows(ma, True, y, moe_gain_at, mo, sq_m, True)
    use_rows(mb, False, x, moe_gain_at, mo, sq_m, True)
    gather_relays(moe)
    for d in (-1, 1):
        use_rows(ma, True, on(y, d), moe_gain_at, mo, sq_m, False)
        use_rows(mb, False, on(x, d), moe_gain_at, mo, sq_m, False)
    gather_last(moe)
    use_rows(ma, True, on(y, 2), moe_gain_at, mo, sq_m, False)
    use_rows(mb, False, on(x, 2), moe_gain_at, mo, sq_m, False)
    for g in moe:
        g.drain()

    scale = lax.rsqrt(sq_m[:, 0:1] * (1.0 / width) + epsilon)
    hidden = (jax.nn.silu(acc_g[...] * scale) * (acc_u[...] * scale)).astype(BF16)
    pair = scatters(
        lambda: hidden, wd, pma, pmb, oma, omb, nma, nmb, o2ma, o2mb, n2ma, n2mb, rsm_s, rsm_r
    )
    got = scatter_all(pair)
    got = jnp.concatenate(got, axis=0)
    outgoing[...] = got.reshape(n_ep, cap, COL).astype(BF16)
    exchange(outgoing, returned, 1)

    @pl.when(owner)
    def _():
        whole(st_back, st_enter, 3, slices - 1).wait_recv()

    @pl.when(not_owner)
    def _():
        whole(st_back, st_enter, 3, slices).wait_recv()

    entering = st_enter[...].reshape(COL, COL).astype(BF16)
    head_out = local_out + lax.dot_general(
        q_enter, entering, (((1,), (1,)), ((), ())), preferred_element_type=F32
    )
    mean = jnp.mean(head_out * head_out, axis=1, keepdims=True)
    gated = head_out * lax.rsqrt(mean + epsilon) * head_gain[...].astype(F32) * gate_out
    gated = gated.astype(BF16)
    pair = scatters(
        lambda: gated, wmix, pxa, pxb, oxa, oxb, nxa, nxb, o2xa, o2xb, n2xa, n2xb, rsx_s, rsx_r
    )
    got = scatter_all(pair)
    mix_out[0:half_x] = got[0].astype(BF16)
    mix_out[half_x : 2 * half_x] = got[1].astype(BF16)

    score0, score1 = places[:, 2:3], places[:, 3:4]
    total = score0 + score1
    slot = lax.broadcasted_iota(jnp.int32, (tok, n_ep * cap), 1).astype(F32)
    weight = jnp.where(slot == places[:, 0:1], score0 / total, 0.0)
    weight = weight + jnp.where(slot == places[:, 1:2], score1 / total, 0.0)
    coarse = weight.astype(BF16)
    fine = (weight - coarse.astype(F32)).astype(BF16)
    whole(outgoing, returned, 1, n_ep - 1).wait_recv()
    results = returned[...].astype(F32).reshape(n_ep * cap, COL).astype(BF16)
    moe_out[...] = (dot(coarse, results) + dot(fine, results)).astype(BF16)

    whole(slots, arrived, 0, n_ep - 1).wait_send()
    whole(outgoing, returned, 1, n_ep - 1).wait_send()

    @pl.when(owner)
    def _():
        whole(st_out, st_in, 2, slices - 1).wait_send()
        whole(st_back, st_back, 3, n_ep - 1).wait_send()

    @pl.when(not_owner)
    def _():
        whole(st_out, st_in, 2, slices).wait_send()


def per_device(n_ep, *args):
    (
        mix_rows,
        mix_gain,
        w_query,
        w_forget,
        w_input,
        w_outgate,
        forget_gap,
        decay_extra,
        head_gain,
        w_mixout,
        moe_rows,
        moe_gain,
        route_ids,
        route_scores,
        w_gate,
        w_up,
        w_down,
    ) = args
    tok_a, tok_b = mix_rows.shape[0], moe_rows.shape[0]
    cap = tok_b * route_ids.shape[1] * 3 // (2 * n_ep)
    rows = n_ep * cap
    hidden = w_gate.shape[2]
    width = w_query.shape[0]
    gains = jnp.stack([mix_gain, moe_gain]).astype(F32).reshape(-1, 1, COL)
    hx, hm = tok_a // 2, rows // 2
    n_tp = SIDE * SIDE
    slices = COL // 8
    vmem = pl.BlockSpec(memory_space=pltpu.VMEM)
    hbm = pl.BlockSpec(memory_space=pltpu.HBM)
    dma = pltpu.SemaphoreType.DMA

    def v(shape, dtype=BF16):
        return pltpu.VMEM(shape, dtype)

    def scatter_buffers(h):
        return [
            v((n_tp, h, COL)),
            v((n_tp, h, COL)),
            v((2, SIDE, h // 2, COL)),
            v((2, SIDE, h // 2, COL)),
            v((2, SIDE, h, COL)),
            v((2, SIDE, h, COL)),
        ]

    def scatter_ends(h):
        return [v((2, h // 2, COL)), v((2, h // 2, COL)), v((2, h, COL)), v((2, h, COL))]

    scratch = [
        v((width, 4 * COL)),
        v((COL, width)),
        v((hidden, width)),
        v((hidden, width)),
        v((hidden, width)),
        v((n_ep, cap, COL)),
        v((n_ep, cap, COL)),
        v((n_ep, cap, COL)),
        v((n_ep, cap, COL)),
        v((tok_b, COL), F32),
        v((n_tp, hx, COL)),
        v((n_tp, hx, COL)),
        v((n_tp, hm, COL)),
        v((n_tp, hm, COL)),
        v((tok_a, 4 * COL), F32),
        v((tok_a, COL), F32),
        v((rows, hidden), F32),
        v((rows, hidden), F32),
        v((rows, COL), F32),
        v((slices, 16, COL)),
        v((n_ep, 16, COL)),
        v((n_ep, 8, COL), F32),
        v((slices, 8, COL), F32),
        *scatter_buffers(hx),
        *scatter_buffers(hm),
        *scatter_ends(hx),
        *scatter_ends(hm),
        dma((8,)),
        dma((4,)),
        dma((4,)),
        dma((2,)),
        dma((2, 20)),
        dma((2,)),
        dma((2, 20)),
        dma((2,)),
        dma((2, 12)),
        dma((2,)),
        dma((2, 12)),
    ]
    return pl.pallas_call(
        functools.partial(step_kernel, n_ep, cap),
        out_shape=[
            jax.ShapeDtypeStruct((tok_a, COL), BF16),
            jax.ShapeDtypeStruct((tok_b, COL), BF16),
        ],
        in_specs=[vmem] * 8 + [hbm] * 8,
        out_specs=[vmem, vmem],
        scratch_shapes=scratch,
        compiler_params=pltpu.CompilerParams(
            collective_id=0, has_side_effects=True, vmem_limit_bytes=60 * 1024 * 1024
        ),
    )(
        mix_rows,
        moe_rows,
        gains,
        forget_gap.reshape(1, COL),
        decay_extra,
        head_gain.reshape(1, COL),
        route_ids.T,
        route_scores.T,
        w_query,
        w_forget,
        w_input,
        w_outgate,
        w_mixout,
        jnp.swapaxes(w_gate, 1, 2),
        jnp.swapaxes(w_up, 1, 2),
        w_down,
    )


def solution(mesh):
    placed = (
        P("ep", "tp"),
        P(),
        P(None, "tp"),
        P(None, "tp"),
        P(None, "tp"),
        P(None, "tp"),
        P("tp"),
        P("tp", "ep"),
        P(),
        P("tp", None),
        P("ep", "tp"),
        P(),
        P("ep", None),
        P("ep", None),
        P("ep", None, "tp"),
        P("ep", None, "tp"),
        P("ep", "tp", None),
    )
    return jax.shard_map(
        functools.partial(per_device, mesh.shape["ep"]),
        mesh=mesh,
        in_specs=placed,
        out_specs=(P("ep", "tp"), P("ep", "tp")),
        check_vma=False,
    )
```

```python
import functools

import jax
import jax.numpy as jnp
from jax import lax
from jax.experimental import pallas as pl
from jax.experimental.pallas import tpu as pltpu
from jax.sharding import PartitionSpec as P

MESH = pl.DeviceIdType.MESH
epsilon = 1e-06
HIGHEST = lax.Precision.HIGHEST
F32, BF16 = jnp.float32, jnp.bfloat16
SIDE = 4
COL = 128
GROUP = SIDE * COL


def dot(a, b):
    return jnp.dot(a, b, preferred_element_type=F32)


def dot_t(a, b):
    return lax.dot_general(a, b, (((1,), (1,)), ((), ())), preferred_element_type=F32)


def step_kernel(
    n_ep,
    cap,
    mix_rows,
    moe_rows,
    mix_gain,
    moe_gain,
    gap,
    decay,
    head_gain,
    ids,
    scores,
    wq_h,
    wf_h,
    wi_h,
    wo_h,
    wmix_h,
    wg_h,
    wu_h,
    wd_h,
    mix_out,
    moe_out,
    wm,
    wmix,
    wg,
    wu,
    wd,
    slots,
    arrived,
    outgoing,
    returned,
    places,
    gains,
    xa,
    xb,
    ma,
    mb,
    acc_x,
    sq_x,
    acc_g,
    acc_u,
    sq_m,
    st_out,
    st_in,
    st_back,
    st_enter,
    pxa,
    pxb,
    oxa,
    oxb,
    nxa,
    nxb,
    pma,
    pmb,
    oma,
    omb,
    nma,
    nmb,
    o2xa,
    o2xb,
    n2xa,
    n2xb,
    o2ma,
    o2mb,
    n2ma,
    n2mb,
    wsem,
    a2a_s,
    a2a_r,
    agx_s,
    agx_r,
    agm_s,
    agm_r,
    rsx_s,
    rsx_r,
    rsm_s,
    rsm_r,
):
    n_z = n_ep // 2
    ep = lax.axis_index("ep")
    tp = lax.axis_index("tp")
    x, y = lax.rem(tp, SIDE), tp // SIDE
    z, core = ep // 2, lax.rem(ep, 2)

    def on(v, d):
        return lax.rem(v + d + SIDE, SIDE)

    x_plus, x_minus = (ep, y * SIDE + on(x, 1)), (ep, y * SIDE + on(x, -1))
    y_plus, y_minus = (ep, on(y, 1) * SIDE + x), (ep, on(y, -1) * SIDE + x)

    loads = [
        pltpu.make_async_copy(src, dst, wsem.at[i])
        for i, (src, dst) in enumerate(
            [
                (wq_h, wm.at[:, 0:COL]),
                (wf_h, wm.at[:, COL : 2 * COL]),
                (wi_h, wm.at[:, 2 * COL : 3 * COL]),
                (wo_h, wm.at[:, 3 * COL : 4 * COL]),
                (wg_h.at[0], wg),
                (wu_h.at[0], wu),
                (wd_h.at[0], wd),
                (wmix_h, wmix),
            ]
        )
    ]
    for load in loads:
        load.start()

    barrier = pltpu.get_barrier_semaphore()
    for peer in (x_plus, x_minus, y_plus, y_minus):
        pl.semaphore_signal(barrier, inc=1, device_id=peer, device_id_type=MESH)

    def greet(o, carry):
        pl.semaphore_signal(
            barrier, inc=1, device_id=(lax.rem(ep + o, n_ep), tp), device_id_type=MESH
        )
        return carry

    lax.fori_loop(1, n_ep, greet, 0)

    gains[0 : SIDE * SIDE] = mix_gain[...].astype(F32).reshape(SIDE * SIDE, 1, COL)
    gains[SIDE * SIDE :] = moe_gain[...].astype(F32).reshape(SIDE * SIDE, 1, COL)

    tok = ids.shape[1]
    id0, id1 = ids[0:1], ids[1:2]
    expert = lax.broadcasted_iota(jnp.int32, (n_ep, tok), 0)
    one0, one1 = expert == id0, expert == id1
    named = jnp.where(one0 | one1, 1.0, 0.0).astype(BF16)
    row = lax.broadcasted_iota(jnp.int32, (tok, tok), 0)
    col = lax.broadcasted_iota(jnp.int32, (tok, tok), 1)
    before = jnp.where(row < col, 1.0, 0.0).astype(BF16)
    rank = dot(named, before)
    place0 = id0.astype(F32) * cap + jnp.sum(jnp.where(one0, rank, 0.0), axis=0, keepdims=True)
    place1 = id1.astype(F32) * cap + jnp.sum(jnp.where(one1, rank, 0.0), axis=0, keepdims=True)
    line = lax.broadcasted_iota(jnp.int32, (COL, tok), 0)
    table = jnp.where(line == 0, place0, place1)
    table = jnp.where(line == 2, scores[0:1], jnp.where(line == 3, scores[1:2], table))
    places[...] = table.T
    slot = lax.broadcasted_iota(jnp.int32, (n_ep * cap, tok), 0).astype(F32)
    pick = jnp.where((slot == place0) | (slot == place1), 1.0, 0.0).astype(BF16)
    slots[...] = dot(pick, moe_rows[...]).reshape(n_ep, cap, COL).astype(BF16)

    half_x = xa.shape[1]
    mine_a, mine_b = y * SIDE + x, x * SIDE + y
    xa[mine_a] = mix_rows[0:half_x]
    xb[mine_b] = mix_rows[half_x : 2 * half_x]

    pl.semaphore_wait(barrier, n_ep - 1 + 4)

    near_z = n_z // 4 - 1

    def partner(u, c, away):
        dz = u - near_z
        return 2 * lax.rem(z + (dz if away else -dz) + 2 * n_z, n_z) + c

    half_ep = n_ep // 2

    def dispatch_copy(i):
        u, c = i // 2, lax.rem(i, 2)
        peer = partner(u, c, False)
        return pltpu.make_async_remote_copy(
            src_ref=slots.at[peer],
            dst_ref=arrived.at[2 * u + core],
            send_sem=a2a_s.at[0],
            recv_sem=a2a_r.at[i // half_ep],
            device_id=(peer, tp),
            device_id_type=MESH,
        )

    def return_copy(i, chunk):
        u, c = i // 2, lax.rem(i, 2)
        peer = partner(u, c, True)
        return pltpu.make_async_remote_copy(
            src_ref=outgoing.at[i],
            dst_ref=returned.at[ep],
            send_sem=a2a_s.at[1],
            recv_sem=a2a_r.at[2 + chunk],
            device_id=(peer, tp),
            device_id_type=MESH,
        )

    own_place = 2 * near_z + core

    def send_all(make, first, count):
        def send(i, carry):
            @pl.when(i != own_place)
            def _():
                make(i).start()

            return carry

        lax.fori_loop(first, first + count, send, 0)

    def whole(src, dst, k, count, r=None):
        return pltpu.make_async_remote_copy(
            src_ref=src.at[pl.ds(0, count)],
            dst_ref=dst.at[pl.ds(0, count)],
            send_sem=a2a_s.at[k],
            recv_sem=a2a_r.at[k if r is None else r],
            device_id=(lax.rem(ep + 1, n_ep), tp),
            device_id_type=MESH,
        )

    class Gather:
        def __init__(self, buf, outer, inner, out_plus, out_minus, in_plus, in_minus, s, r):
            self.buf, self.outer, self.inner = buf, outer, inner
            self.op, self.om, self.ip, self.im = out_plus, out_minus, in_plus, in_minus
            self.s, self.r = s, r
            self.h = buf.shape[1]

        def at(self, do, di):
            return on(self.outer, do) * SIDE + on(self.inner, di)

        def copy(self, block, rows, sem, to):
            ref = self.buf.at[block] if rows is None else self.buf.at[block, pl.ds(*rows)]
            return pltpu.make_async_remote_copy(
                src_ref=ref,
                dst_ref=ref,
                send_sem=self.s,
                recv_sem=self.r.at[sem],
                device_id=to,
                device_id_type=MESH,
            )

        def first(self):
            q = self.h // 2
            self.lo, self.hi = (0, q), (q, q)
            self.copy(self.at(0, 0), None, 0, self.ip).start()
            self.copy(self.at(0, 0), None, 1, self.im).start()

        def cross(self, di, sem):
            self.copy(self.at(0, di), None, sem, self.op).start()
            self.copy(self.at(0, di), None, sem + 1, self.om).start()

        def near(self):
            self.copy(self.at(0, -1), None, 0, self.ip).wait_recv()
            self.copy(self.at(0, -1), self.lo, 2, self.ip).start()
            self.copy(self.at(0, 1), None, 1, self.im).wait_recv()
            self.copy(self.at(0, 1), self.hi, 3, self.im).start()

        def far(self):
            self.copy(self.at(0, 2), self.lo, 2, self.ip).wait_recv()
            self.copy(self.at(0, 2), self.hi, 3, self.im).wait_recv()

        def relay(self, di, sem):
            self.copy(self.at(-1, di), None, sem, self.op).wait_recv()
            self.copy(self.at(-1, di), self.lo, sem + 2, self.op).start()
            self.copy(self.at(1, di), None, sem + 1, self.om).wait_recv()
            self.copy(self.at(1, di), self.hi, sem + 3, self.om).start()

        def last(self, di, sem):
            self.copy(self.at(2, di), self.lo, sem + 2, self.op).wait_recv()
            self.copy(self.at(2, di), self.hi, sem + 3, self.om).wait_recv()

        def drain(self):
            ref = self.buf.at[pl.ds(0, SIDE * SIDE - 1)]
            pltpu.make_async_remote_copy(
                src_ref=ref,
                dst_ref=ref,
                send_sem=self.s,
                recv_sem=self.r.at[0],
                device_id=self.op,
                device_id_type=MESH,
            ).wait_send()

    def gathers(a, b, s, r):
        return (
            Gather(a, y, x, y_plus, y_minus, x_plus, x_minus, s.at[0], r.at[0]),
            Gather(b, x, y, x_plus, x_minus, y_plus, y_minus, s.at[1], r.at[1]),
        )

    crossings = ((0, 4), (-1, 8), (1, 12), (2, 16))

    def gather_start(pair):
        for g in pair:
            g.first()
        for g in pair:
            g.cross(0, 4)

    def gather_near(pair):
        for g in pair:
            g.near()
        for g in pair:
            g.cross(-1, 8)
            g.cross(1, 12)
        for g in pair:
            g.relay(0, 4)

    def gather_far(pair):
        for g in pair:
            g.far()
            g.cross(2, 16)
        for g in pair:
            g.relay(-1, 8)
            g.relay(1, 12)

    def gather_relays(pair):
        for g in pair:
            g.relay(2, 16)

    def gather_last(pair):
        for di, sem in crossings:
            for g in pair:
                g.last(di, sem)

    ones = jnp.ones((GROUP, COL), BF16)

    def features(is_a, group, j):
        return group * SIDE + j if is_a else j * SIDE + group

    def weight_rows(ref, is_a, group):
        if is_a:
            return ref[pl.ds(pl.multiple_of(group * GROUP, GROUP), GROUP), :]
        return jnp.concatenate(
            [
                ref[pl.ds(pl.multiple_of(features(False, group, j) * COL, COL), COL), :]
                for j in range(SIDE)
            ],
            axis=0,
        )

    def weight_columns(ref, is_a, group):
        if is_a:
            return ref[:, pl.ds(pl.multiple_of(group * GROUP, GROUP), GROUP)]
        return jnp.concatenate(
            [
                ref[:, pl.ds(pl.multiple_of(features(False, group, j) * COL, COL), COL)]
                for j in range(SIDE)
            ],
            axis=1,
        )

    def use_rows(buf, is_a, group, gain_at, outs, sq, start, at=0):
        h = buf.shape[1]
        scaled, squares = [], []
        for j in range(SIDE):
            part = buf[group * SIDE + j].astype(F32)
            scaled.append((part * gains[gain_at + features(is_a, group, j)]).astype(BF16))
            squares.append((part * part).astype(BF16))
        scaled, squares = jnp.concatenate(scaled, axis=1), jnp.concatenate(squares, axis=1)
        rows = pl.ds(at if is_a else at + h, h)
        found = [(sq, dot(squares, ones))]
        for ref, acc in outs:
            if ref.shape[0] > ref.shape[1]:
                found.append((acc, dot(scaled, weight_rows(ref, is_a, group))))
            else:
                found.append((acc, dot_t(scaled, weight_columns(ref, is_a, group))))
        for acc, got in found:
            acc[rows, :] = got if start else acc[rows, :] + got

    class Scatter:
        def __init__(self, p, o1, n1, o2, n2, outer, inner, op, om, ip, im, s, r, make):
            self.p, self.o1, self.n1, self.o2, self.n2 = p, o1, n1, o2, n2
            self.outer, self.inner = outer, inner
            self.op, self.om, self.ip, self.im = op, om, ip, im
            self.s, self.r, self.make = s, r, make
            self.h = p.shape[1]
            self.q = self.h // 2
            self.lo, self.hi = pl.ds(0, self.q), pl.ds(self.q, self.q)

        def copy(self, src, dst, sem, to):
            return pltpu.make_async_remote_copy(
                src_ref=src,
                dst_ref=dst,
                send_sem=self.s,
                recv_sem=self.r.at[sem],
                device_id=to,
                device_id_type=MESH,
            )

        def produce(self, do):
            group = on(self.outer, do)
            got = self.make(group)
            for j in range(SIDE):
                self.p[group * SIDE + j] = got[:, j * COL : (j + 1) * COL].astype(BF16)

        def group(self, do, rows):
            return self.p.at[pl.ds(on(self.outer, do) * SIDE, SIDE), rows]

        def block(self, di, rows):
            return self.p.at[self.outer * SIDE + on(self.inner, di), rows]

        def leg1(self, name):
            return dict(
                a=lambda: self.copy(self.group(2, self.lo), self.o1.at[0], 0, self.op),
                b=lambda: self.copy(self.group(2, self.hi), self.o1.at[1], 1, self.om),
                c=lambda: self.copy(self.group(1, self.hi), self.n1.at[0, :, self.hi], 2, self.op),
                d=lambda: self.copy(self.group(-1, self.lo), self.n1.at[1, :, self.lo], 3, self.om),
                e=lambda: self.copy(self.group(1, self.lo), self.n1.at[0, :, self.lo], 4, self.op),
                f=lambda: self.copy(self.group(-1, self.hi), self.n1.at[1, :, self.hi], 5, self.om),
            )[name]()

        def leg2(self, name):
            return dict(
                a=lambda: self.copy(self.block(2, self.lo), self.o2.at[0], 6, self.ip),
                b=lambda: self.copy(self.block(2, self.hi), self.o2.at[1], 7, self.im),
                c=lambda: self.copy(self.block(1, self.hi), self.n2.at[0, self.hi], 8, self.ip),
                d=lambda: self.copy(self.block(-1, self.lo), self.n2.at[1, self.lo], 9, self.im),
                e=lambda: self.copy(self.block(1, self.lo), self.n2.at[0, self.lo], 10, self.ip),
                f=lambda: self.copy(self.block(-1, self.hi), self.n2.at[1, self.hi], 11, self.im),
            )[name]()

        def start1(self):
            self.produce(2)
            self.leg1("a").start()
            self.leg1("b").start()

        def direct1(self):
            self.produce(1)
            self.leg1("c").start()
            self.produce(-1)
            self.leg1("d").start()

        def add(self, dst, src):
            dst[...] = (dst[...].astype(F32) + src[...].astype(F32)).astype(BF16)

        def relay1(self):
            self.leg1("a").wait_recv()
            self.add(self.group(1, self.lo), self.o1.at[0])
            self.leg1("e").start()
            self.leg1("b").wait_recv()
            self.add(self.group(-1, self.hi), self.o1.at[1])
            self.leg1("f").start()

        def settle1(self):
            for leg in "cdef":
                self.leg1(leg).wait_recv()
            here = self.p.at[pl.ds(self.outer * SIDE, SIDE)]
            here[...] = (
                here[...].astype(F32) + self.n1[0].astype(F32) + self.n1[1].astype(F32)
            ).astype(BF16)
            for leg in "abcd":
                self.leg2(leg).start()

        def relay2(self):
            self.leg2("a").wait_recv()
            self.add(self.block(1, self.lo), self.o2.at[0])
            self.leg2("e").start()
            self.leg2("b").wait_recv()
            self.add(self.block(-1, self.hi), self.o2.at[1])
            self.leg2("f").start()

        def settle2(self):
            for leg in "cdef":
                self.leg2(leg).wait_recv()
            mine = self.p[self.outer * SIDE + self.inner].astype(F32)
            return mine + self.n2[0].astype(F32) + self.n2[1].astype(F32)

        def drain(self):
            ref = self.p.at[pl.ds(0, SIDE * SIDE - 1)]
            self.copy(ref, ref, 0, self.op).wait_send()

    def scatters(left, w, pa, pb, oa, ob, na, nb, o2a, o2b, n2a, n2b, s, r):
        h = pa.shape[1]

        def make_a(group):
            return dot(left()[0:h], weight_columns(w, True, group))

        def make_b(group):
            return dot(left()[h : 2 * h], weight_columns(w, False, group))

        return (
            Scatter(
                pa, oa, na, o2a, n2a, y, x, y_plus, y_minus, x_plus, x_minus, s.at[0], r.at[0], make_a
            ),
            Scatter(
                pb, ob, nb, o2b, n2b, x, y, x_plus, x_minus, y_plus, y_minus, s.at[1], r.at[1], make_b
            ),
        )

    def scatter_start(pair):
        for g in pair:
            g.start1()
        for g in pair:
            g.direct1()

    def scatter_relay(pair):
        for g in pair:
            g.relay1()
        for g in pair:
            g.produce(0)

    def scatter_settle(pair):
        for g in pair:
            g.settle1()

    def scatter_relay2(pair):
        for g in pair:
            g.relay2()

    def scatter_end(pair):
        got = [g.settle2() for g in pair]
        for g in pair:
            g.drain()
        return got

    live = {}
    mix = gathers(xa, xb, agx_s, agx_r)
    xo = [(wm, acc_x)]

    def x_start():
        gather_start(mix)

    def x_near():
        gather_near(mix)

    def x_far():
        gather_far(mix)
        for load in loads[0:4]:
            load.wait()
        use_rows(xa, True, y, 0, xo, sq_x, True)
        use_rows(xb, False, x, 0, xo, sq_x, True)

    def x_relays():
        gather_relays(mix)
        for d in (-1, 1):
            use_rows(xa, True, on(y, d), 0, xo, sq_x, False)
            use_rows(xb, False, on(x, d), 0, xo, sq_x, False)

    width = SIDE * SIDE * COL

    def x_last():
        gather_last(mix)
        use_rows(xa, True, on(y, 2), 0, xo, sq_x, False)
        use_rows(xb, False, on(x, 2), 0, xo, sq_x, False)
        for g in mix:
            g.drain()

    def recurrence():
        scale = lax.rsqrt(sq_x[...] * (1.0 / width) + epsilon)
        query = jax.nn.silu(acc_x[:, 0:COL] * scale)
        key = gap[...] * jax.nn.sigmoid(-(acc_x[:, COL : 2 * COL] * scale))
        value = (acc_x[:, 2 * COL : 3 * COL] * scale).astype(BF16)
        gate_out = jax.nn.silu(acc_x[:, 3 * COL : 4 * COL] * scale)
        extra = jnp.broadcast_to(decay[...], (COL, decay.shape[1])).T
        log_forget = jnp.log1p(-key) + extra
        part = half_x
        row = lax.broadcasted_iota(jnp.int32, (part, part), 0)
        col = lax.broadcasted_iota(jnp.int32, (part, part), 1)
        causal = row >= col
        lower = jnp.where(causal, 1.0, 0.0)
        outs, running, states, ends = [], [], [], []
        for c in range(2):
            rows = slice(c * part, (c + 1) * part)
            run = jnp.dot(lower, log_forget[rows], precision=HIGHEST, preferred_element_type=F32)
            mid, end = run[part // 2 - 1 : part // 2], run[part - 1 : part]
            q_in = (query[rows] * jnp.exp(run - mid)).astype(BF16)
            k_in = (key[rows] * jnp.exp(mid - run)).astype(BF16)
            near = lax.dot_general(q_in, k_in, (((1,), (1,)), ((), ())), preferred_element_type=F32)
            near = jnp.where(causal, near, 0.0).astype(BF16)
            outs.append(dot(near, value[rows]))
            k_end = (key[rows] * jnp.exp(end - run)).astype(BF16)
            states.append(
                lax.dot_general(value[rows], k_end, (((0,), (0,)), ((), ())), preferred_element_type=F32)
            )
            running.append(run)
            ends.append(end)
        q_second = (query[part:] * jnp.exp(running[1])).astype(BF16)
        outs[1] = outs[1] + lax.dot_general(
            q_second, states[0].astype(BF16), (((1,), (1,)), ((), ())), preferred_element_type=F32
        )
        state = states[0] * jnp.exp(ends[1]) + states[1]
        passing = jnp.exp(ends[0] + ends[1])
        q_enter = jnp.concatenate(
            [
                (query[:part] * jnp.exp(running[0])).astype(BF16),
                (query[part:] * jnp.exp(ends[0] + running[1])).astype(BF16),
            ],
            axis=0,
        )
        local_out = jnp.concatenate(outs, axis=0)
        st_out[...] = jnp.concatenate(
            [
                state.reshape(slices, 8, COL),
                jnp.broadcast_to(passing.reshape(1, 1, COL), (slices, 8, COL)),
            ],
            axis=1,
        ).astype(BF16)


        def to_owner(k, carry):
            peer = 2 * k + lax.rem(k, 2)

            @pl.when(peer != ep)
            def _():
                pltpu.make_async_remote_copy(
                    src_ref=st_out.at[k],
                    dst_ref=st_in.at[ep],
                    send_sem=a2a_s.at[2],
                    recv_sem=a2a_r.at[4],
                    device_id=(peer, tp),
                    device_id_type=MESH,
                ).start()

            return carry

        lax.fori_loop(0, slices, to_owner, 0)

        @pl.when(owner)
        def _():
            st_in[ep] = st_out[z]
        live.update(local_out=local_out, q_enter=q_enter, gate_out=gate_out)

    slices = COL // 8
    owner = core == lax.rem(z, 2)
    not_owner = jnp.logical_not(owner)

    def chain_states():
        @pl.when(owner)
        def _():
            whole(st_in, st_in, 2, n_ep - 1, 4).wait_recv()

            def chain(j, entering):
                block = st_in[j].astype(F32)
                st_back[j] = entering
                return block[8:16] * entering + block[0:8]

            lax.fori_loop(0, n_ep, chain, jnp.zeros((8, COL), F32))

            def give(o, carry):
                peer = lax.rem(ep + o, n_ep)
                pltpu.make_async_remote_copy(
                    src_ref=st_back.at[peer],
                    dst_ref=st_enter.at[z],
                    send_sem=a2a_s.at[3],
                    recv_sem=a2a_r.at[5],
                    device_id=(peer, tp),
                    device_id_type=MESH,
                ).start()
                return carry

            lax.fori_loop(1, n_ep, give, 0)
            st_enter[z] = st_back[ep]

    moe_gain_at = SIDE * SIDE
    half_m = ma.shape[2]
    chunks = []

    class Chunk:
        def __init__(self, c):
            self.c = c
            self.a, self.b = ma.at[c], mb.at[c]
            self.pair = gathers(self.a, self.b, agm_s.at[c], agm_r.at[c])
            self.at = 2 * half_m * c
            self.outs = [(wg, acc_g), (wu, acc_u)]

        def use(self, d, start):
            use_rows(self.a, True, on(y, d), moe_gain_at, self.outs, sq_m, start, self.at)
            use_rows(self.b, False, on(x, d), moe_gain_at, self.outs, sq_m, start, self.at)

        def start(self):
            whole(slots, arrived, 0, half_ep - (1 if self.c == 0 else 0), self.c).wait_recv()
            got = arrived[half_ep * self.c : half_ep * (self.c + 1)].astype(F32)
            got = got.reshape(2 * half_m, COL).astype(BF16)
            self.a[mine_a] = got[0:half_m]
            self.b[mine_b] = got[half_m:]
            gather_start(self.pair)

        def near(self):
            gather_near(self.pair)

        def far(self):
            gather_far(self.pair)
            if self.c == 0:
                for load in loads[4:6]:
                    load.wait()
            self.use(0, True)

        def relays(self):
            gather_relays(self.pair)
            self.use(-1, False)
            self.use(1, False)

        def last(self):
            gather_last(self.pair)
            self.use(2, False)
            for g in self.pair:
                g.drain()

        def experts(self):
            if self.c == 0:
                for load in loads[6:]:
                    load.wait()
            rows = pl.ds(self.at, 2 * half_m)
            scale = lax.rsqrt(sq_m[rows, 0:1] * (1.0 / width) + epsilon)
            hidden = (jax.nn.silu(acc_g[rows, :] * scale) * (acc_u[rows, :] * scale)).astype(BF16)
            refs = [ref.at[self.c] for ref in (pma, pmb, oma, omb, nma, nmb, o2ma, o2mb, n2ma, n2mb)]
            self.sums = scatters(lambda: hidden, wd, *refs, rsm_s.at[self.c], rsm_r.at[self.c])
            scatter_start(self.sums)

        def sum_relay(self):
            scatter_relay(self.sums)

        def sum_settle(self):
            scatter_settle(self.sums)

        def sum_relay2(self):
            scatter_relay2(self.sums)

        def give_back(self):
            got = jnp.concatenate(scatter_end(self.sums), axis=0)
            first = half_ep * self.c
            outgoing[first : first + half_ep] = got.reshape(half_ep, cap, COL).astype(BF16)
            send_all(lambda i: return_copy(i, self.c), first, half_ep)
            if self.c == 0:
                returned[ep] = outgoing[own_place]

    near_chunk, far_chunk = Chunk(0), Chunk(1)

    def x_sum_start():
        @pl.when(owner)
        def _():
            whole(st_back, st_enter, 3, slices - 1, 5).wait_recv()

        @pl.when(not_owner)
        def _():
            whole(st_back, st_enter, 3, slices, 5).wait_recv()

        entering = st_enter[...].reshape(COL, COL).astype(BF16)
        head_out = live["local_out"] + lax.dot_general(
            live["q_enter"], entering, (((1,), (1,)), ((), ())), preferred_element_type=F32
        )
        mean = jnp.mean(head_out * head_out, axis=1, keepdims=True)
        gated = head_out * lax.rsqrt(mean + epsilon) * head_gain[...].astype(F32) * live["gate_out"]
        gated = gated.astype(BF16)
        refs = (pxa, pxb, oxa, oxb, nxa, nxb, o2xa, o2xb, n2xa, n2xb)
        live["sums"] = scatters(lambda: gated, wmix, *refs, rsx_s, rsx_r)
        scatter_start(live["sums"])

    def x_sum_relay():
        scatter_relay(live["sums"])

    def x_sum_settle():
        scatter_settle(live["sums"])

    def x_sum_relay2():
        scatter_relay2(live["sums"])

    def x_store():
        got = scatter_end(live["sums"])
        mix_out[0:half_x] = got[0].astype(BF16)
        mix_out[half_x : 2 * half_x] = got[1].astype(BF16)

    def weigh():
        score0, score1 = places[:, 2:3], places[:, 3:4]
        total = score0 + score1
        slot = lax.broadcasted_iota(jnp.int32, (tok, n_ep * cap), 1).astype(F32)
        weight = jnp.where(slot == places[:, 0:1], score0 / total, 0.0)
        weight = weight + jnp.where(slot == places[:, 1:2], score1 / total, 0.0)
        coarse = weight.astype(BF16)
        fine = (weight - coarse.astype(F32)).astype(BF16)
        live.update(coarse=coarse, fine=fine)

    def combine():
        whole(outgoing, returned, 1, half_ep - 1, 2).wait_recv()
        whole(outgoing, returned, 1, half_ep, 3).wait_recv()
        results = returned[...].astype(F32).reshape(n_ep * cap, COL).astype(BF16)
        moe_out[...] = (dot(live["coarse"], results) + dot(live["fine"], results)).astype(BF16)

    send_all(dispatch_copy, 0, half_ep)
    x_start()
    arrived[own_place] = slots[ep]
    x_near()
    send_all(dispatch_copy, half_ep, half_ep)
    x_far()
    near_chunk.start()
    x_relays()
    near_chunk.near()
    x_last()
    near_chunk.far()
    far_chunk.start()
    recurrence()
    near_chunk.relays()
    far_chunk.near()
    near_chunk.last()
    far_chunk.far()
    near_chunk.experts()
    chain_states()
    far_chunk.relays()
    far_chunk.last()
    far_chunk.experts()
    near_chunk.sum_relay()
    far_chunk.sum_relay()
    far_chunk.sum_settle()
    near_chunk.sum_settle()
    x_sum_start()
    far_chunk.sum_relay2()
    x_sum_relay()
    far_chunk.give_back()
    near_chunk.sum_relay2()
    x_sum_settle()
    near_chunk.give_back()
    x_sum_relay2()
    weigh()
    x_store()
    combine()

    whole(slots, arrived, 0, n_ep - 1).wait_send()
    whole(outgoing, returned, 1, n_ep - 1).wait_send()

    @pl.when(owner)
    def _():
        whole(st_out, st_in, 2, slices - 1).wait_send()
        whole(st_back, st_back, 3, n_ep - 1).wait_send()

    @pl.when(not_owner)
    def _():
        whole(st_out, st_in, 2, slices).wait_send()


def per_device(n_ep, *args):
    (
        mix_rows,
        mix_gain,
        w_query,
        w_forget,
        w_input,
        w_outgate,
        forget_gap,
        decay_extra,
        head_gain,
        w_mixout,
        moe_rows,
        moe_gain,
        route_ids,
        route_scores,
        w_gate,
        w_up,
        w_down,
    ) = args
    tok_a, tok_b = mix_rows.shape[0], moe_rows.shape[0]
    cap = tok_b * route_ids.shape[1] * 3 // (2 * n_ep)
    rows = n_ep * cap
    hidden = w_gate.shape[2]
    width = w_query.shape[0]
    hx, hm = tok_a // 2, rows // 4
    n_tp = SIDE * SIDE
    slices = COL // 8
    vmem = pl.BlockSpec(memory_space=pltpu.VMEM)
    hbm = pl.BlockSpec(memory_space=pltpu.HBM)
    dma = pltpu.SemaphoreType.DMA

    def v(shape, dtype=BF16):
        return pltpu.VMEM(shape, dtype)

    def scatter_buffers(h, n=()):
        return [
            v((*n, n_tp, h, COL)),
            v((*n, n_tp, h, COL)),
            v((*n, 2, SIDE, h // 2, COL)),
            v((*n, 2, SIDE, h // 2, COL)),
            v((*n, 2, SIDE, h, COL)),
            v((*n, 2, SIDE, h, COL)),
        ]

    def scatter_ends(h, n=()):
        return [v((*n, 2, h // 2, COL)), v((*n, 2, h // 2, COL)), v((*n, 2, h, COL)), v((*n, 2, h, COL))]

    scratch = [
        v((width, 4 * COL)),
        v((COL, width)),
        v((hidden, width)),
        v((hidden, width)),
        v((hidden, width)),
        v((n_ep, cap, COL)),
        v((n_ep, cap, COL)),
        v((n_ep, cap, COL)),
        v((n_ep, cap, COL)),
        v((tok_b, COL), F32),
        v((2 * n_tp, 1, COL), F32),
        v((n_tp, hx, COL)),
        v((n_tp, hx, COL)),
        v((2, n_tp, hm, COL)),
        v((2, n_tp, hm, COL)),
        v((tok_a, 4 * COL), F32),
        v((tok_a, COL), F32),
        v((rows, hidden), F32),
        v((rows, hidden), F32),
        v((rows, COL), F32),
        v((slices, 16, COL)),
        v((n_ep, 16, COL)),
        v((n_ep, 8, COL), F32),
        v((slices, 8, COL), F32),
        *scatter_buffers(hx),
        *scatter_buffers(hm, (2,)),
        *scatter_ends(hx),
        *scatter_ends(hm, (2,)),
        dma((8,)),
        dma((4,)),
        dma((6,)),
        dma((2,)),
        dma((2, 20)),
        dma((2, 2)),
        dma((2, 2, 20)),
        dma((2,)),
        dma((2, 12)),
        dma((2, 2)),
        dma((2, 2, 12)),
    ]
    return pl.pallas_call(
        functools.partial(step_kernel, n_ep, cap),
        out_shape=[
            jax.ShapeDtypeStruct((tok_a, COL), BF16),
            jax.ShapeDtypeStruct((tok_b, COL), BF16),
        ],
        in_specs=[vmem] * 9 + [hbm] * 8,
        out_specs=[vmem, vmem],
        scratch_shapes=scratch,
        compiler_params=pltpu.CompilerParams(
            collective_id=0, has_side_effects=True, vmem_limit_bytes=60 * 1024 * 1024
        ),
    )(
        mix_rows,
        moe_rows,
        mix_gain.reshape(-1, COL),
        moe_gain.reshape(-1, COL),
        forget_gap.reshape(1, COL),
        decay_extra,
        head_gain.reshape(1, COL),
        route_ids.T,
        route_scores.T,
        w_query,
        w_forget,
        w_input,
        w_outgate,
        w_mixout,
        jnp.swapaxes(w_gate, 1, 2),
        jnp.swapaxes(w_up, 1, 2),
        w_down,
    )


def solution(mesh):
    placed = (
        P("ep", "tp"),
        P(),
        P(None, "tp"),
        P(None, "tp"),
        P(None, "tp"),
        P(None, "tp"),
        P("tp"),
        P("tp", "ep"),
        P(),
        P("tp", None),
        P("ep", "tp"),
        P(),
        P("ep", None),
        P("ep", None),
        P("ep", None, "tp"),
        P("ep", None, "tp"),
        P("ep", "tp", None),
    )
    return jax.shard_map(
        functools.partial(per_device, mesh.shape["ep"]),
        mesh=mesh,
        in_specs=placed,
        out_specs=(P("ep", "tp"), P("ep", "tp")),
        check_vma=False,
    )
```

```python
import functools

import jax
import jax.numpy as jnp
from jax import lax
from jax.experimental import pallas as pl
from jax.experimental.pallas import tpu as pltpu
from jax.sharding import PartitionSpec as P

MESH = pl.DeviceIdType.MESH
epsilon = 1e-06
HIGHEST = lax.Precision.HIGHEST
F32, BF16 = jnp.float32, jnp.bfloat16
SIDE = 4
COL = 128
GROUP = SIDE * COL


def dot(a, b):
    return jnp.dot(a, b, preferred_element_type=F32)


def dot_t(a, b):
    return lax.dot_general(a, b, (((1,), (1,)), ((), ())), preferred_element_type=F32)


def step_kernel(
    n_ep,
    cap,
    mix_rows_h,
    moe_rows_h,
    mix_gain_h,
    moe_gain_h,
    gap_h,
    decay_h,
    head_gain_h,
    ids_h,
    scores_h,
    wq_h,
    wf_h,
    wi_h,
    wo_h,
    wmix_h,
    wg_h,
    wu_h,
    wd_h,
    mix_out_h,
    moe_out_h,
    mix_rows,
    moe_rows,
    mix_gain,
    moe_gain,
    gap,
    decay,
    head_gain,
    ids,
    scores,
    mix_out,
    moe_out,
    wm,
    wmix,
    wg,
    wu,
    wd,
    slots,
    arrived,
    outgoing,
    returned,
    places,
    gains,
    xa,
    xb,
    ma,
    mb,
    acc_x,
    sq_x,
    acc_g,
    acc_u,
    sq_m,
    st_out,
    st_in,
    st_back,
    st_enter,
    pxa,
    pxb,
    oxa,
    oxb,
    nxa,
    nxb,
    pma,
    pmb,
    oma,
    omb,
    nma,
    nmb,
    o2xa,
    o2xb,
    n2xa,
    n2xb,
    o2ma,
    o2mb,
    n2ma,
    n2mb,
    isem,
    osem,
    wsem,
    a2a_s,
    a2a_r,
    agx_s,
    agx_r,
    agm_s,
    agm_r,
    rsx_s,
    rsx_r,
    rsm_s,
    rsm_r,
):
    n_z = n_ep // 2
    ep = lax.axis_index("ep")
    tp = lax.axis_index("tp")
    x, y = lax.rem(tp, SIDE), tp // SIDE
    z, core = ep // 2, lax.rem(ep, 2)

    def on(v, d):
        return lax.rem(v + d + SIDE, SIDE)

    x_plus, x_minus = (ep, y * SIDE + on(x, 1)), (ep, y * SIDE + on(x, -1))
    y_plus, y_minus = (ep, on(y, 1) * SIDE + x), (ep, on(y, -1) * SIDE + x)

    barrier = pltpu.get_barrier_semaphore()
    for peer in (x_plus, x_minus, y_plus, y_minus):
        pl.semaphore_signal(barrier, inc=1, device_id=peer, device_id_type=MESH)

    def greet(o, carry):
        pl.semaphore_signal(
            barrier, inc=1, device_id=(lax.rem(ep + o, n_ep), tp), device_id_type=MESH
        )
        return carry

    lax.fori_loop(1, n_ep, greet, 0)

    firsts = [
        pltpu.make_async_copy(src, dst, isem.at[i])
        for i, (src, dst) in enumerate(
            [
                (ids_h, ids),
                (scores_h, scores),
                (moe_rows_h, moe_rows),
                (mix_rows_h, mix_rows),
                (mix_gain_h, mix_gain),
                (moe_gain_h, moe_gain),
                (gap_h, gap),
                (decay_h, decay),
                (head_gain_h, head_gain),
            ]
        )
    ]
    for first in firsts:
        first.start()
    loads = [
        pltpu.make_async_copy(src, dst, wsem.at[i])
        for i, (src, dst) in enumerate(
            [
                (wq_h, wm.at[:, 0:COL]),
                (wf_h, wm.at[:, COL : 2 * COL]),
                (wi_h, wm.at[:, 2 * COL : 3 * COL]),
                (wo_h, wm.at[:, 3 * COL : 4 * COL]),
                (wg_h.at[0], wg),
                (wu_h.at[0], wu),
                (wd_h.at[0], wd),
                (wmix_h, wmix),
            ]
        )
    ]
    for load in loads:
        load.start()

    for first in firsts:
        first.wait()

    gains[0 : SIDE * SIDE] = mix_gain[...].astype(F32).reshape(SIDE * SIDE, 1, COL)
    gains[SIDE * SIDE :] = moe_gain[...].astype(F32).reshape(SIDE * SIDE, 1, COL)

    tok = ids.shape[1]
    id0, id1 = ids[0:1], ids[1:2]
    expert = lax.broadcasted_iota(jnp.int32, (n_ep, tok), 0)
    one0, one1 = expert == id0, expert == id1
    named = jnp.where(one0 | one1, 1.0, 0.0).astype(BF16)
    row = lax.broadcasted_iota(jnp.int32, (tok, tok), 0)
    col = lax.broadcasted_iota(jnp.int32, (tok, tok), 1)
    before = jnp.where(row < col, 1.0, 0.0).astype(BF16)
    rank = dot(named, before)
    place0 = id0.astype(F32) * cap + jnp.sum(jnp.where(one0, rank, 0.0), axis=0, keepdims=True)
    place1 = id1.astype(F32) * cap + jnp.sum(jnp.where(one1, rank, 0.0), axis=0, keepdims=True)
    line = lax.broadcasted_iota(jnp.int32, (COL, tok), 0)
    table = jnp.where(line == 0, place0, place1)
    table = jnp.where(line == 2, scores[0:1], jnp.where(line == 3, scores[1:2], table))
    places[...] = table.T
    slot = lax.broadcasted_iota(jnp.int32, (n_ep * cap, tok), 0).astype(F32)
    pick = jnp.where((slot == place0) | (slot == place1), 1.0, 0.0).astype(BF16)
    slots[...] = dot(pick, moe_rows[...]).reshape(n_ep, cap, COL).astype(BF16)

    half_x = xa.shape[1]
    mine_a, mine_b = y * SIDE + x, x * SIDE + y
    xa[mine_a] = mix_rows[0:half_x]
    xb[mine_b] = mix_rows[half_x : 2 * half_x]

    pl.semaphore_wait(barrier, n_ep - 1 + 4)

    near_z = n_z // 4 - 1

    def partner(u, c, away):
        dz = u - near_z
        return 2 * lax.rem(z + (dz if away else -dz) + 2 * n_z, n_z) + c

    half_ep = n_ep // 2

    def dispatch_copy(i):
        u, c = i // 2, lax.rem(i, 2)
        peer = partner(u, c, False)
        return pltpu.make_async_remote_copy(
            src_ref=slots.at[peer],
            dst_ref=arrived.at[2 * u + core],
            send_sem=a2a_s.at[0],
            recv_sem=a2a_r.at[i // half_ep],
            device_id=(peer, tp),
            device_id_type=MESH,
        )

    def return_copy(i, chunk):
        u, c = i // 2, lax.rem(i, 2)
        peer = partner(u, c, True)
        return pltpu.make_async_remote_copy(
            src_ref=outgoing.at[i],
            dst_ref=returned.at[ep],
            send_sem=a2a_s.at[1],
            recv_sem=a2a_r.at[2 + chunk],
            device_id=(peer, tp),
            device_id_type=MESH,
        )

    own_place = 2 * near_z + core

    def send_all(make, first, count):
        def send(i, carry):
            @pl.when(i != own_place)
            def _():
                make(i).start()

            return carry

        lax.fori_loop(first, first + count, send, 0)

    def whole(src, dst, k, count, r=None):
        return pltpu.make_async_remote_copy(
            src_ref=src.at[pl.ds(0, count)],
            dst_ref=dst.at[pl.ds(0, count)],
            send_sem=a2a_s.at[k],
            recv_sem=a2a_r.at[k if r is None else r],
            device_id=(lax.rem(ep + 1, n_ep), tp),
            device_id_type=MESH,
        )

    class Gather:
        def __init__(self, buf, outer, inner, out_plus, out_minus, in_plus, in_minus, s, r):
            self.buf, self.outer, self.inner = buf, outer, inner
            self.op, self.om, self.ip, self.im = out_plus, out_minus, in_plus, in_minus
            self.s, self.r = s, r
            self.h = buf.shape[1]

        def at(self, do, di):
            return on(self.outer, do) * SIDE + on(self.inner, di)

        def copy(self, block, rows, sem, to):
            ref = self.buf.at[block] if rows is None else self.buf.at[block, pl.ds(*rows)]
            return pltpu.make_async_remote_copy(
                src_ref=ref,
                dst_ref=ref,
                send_sem=self.s,
                recv_sem=self.r.at[sem],
                device_id=to,
                device_id_type=MESH,
            )

        def first(self):
            q = self.h // 2
            self.lo, self.hi = (0, q), (q, q)
            self.copy(self.at(0, 0), None, 0, self.ip).start()
            self.copy(self.at(0, 0), None, 1, self.im).start()

        def cross(self, di, sem):
            self.copy(self.at(0, di), None, sem, self.op).start()
            self.copy(self.at(0, di), None, sem + 1, self.om).start()

        def near(self):
            self.copy(self.at(0, -1), None, 0, self.ip).wait_recv()
            self.copy(self.at(0, -1), self.lo, 2, self.ip).start()
            self.copy(self.at(0, 1), None, 1, self.im).wait_recv()
            self.copy(self.at(0, 1), self.hi, 3, self.im).start()

        def far(self):
            self.copy(self.at(0, 2), self.lo, 2, self.ip).wait_recv()
            self.copy(self.at(0, 2), self.hi, 3, self.im).wait_recv()

        def relay(self, di, sem):
            self.copy(self.at(-1, di), None, sem, self.op).wait_recv()
            self.copy(self.at(-1, di), self.lo, sem + 2, self.op).start()
            self.copy(self.at(1, di), None, sem + 1, self.om).wait_recv()
            self.copy(self.at(1, di), self.hi, sem + 3, self.om).start()

        def last(self, di, sem):
            self.copy(self.at(2, di), self.lo, sem + 2, self.op).wait_recv()
            self.copy(self.at(2, di), self.hi, sem + 3, self.om).wait_recv()

        def drain(self):
            ref = self.buf.at[pl.ds(0, SIDE * SIDE - 1)]
            pltpu.make_async_remote_copy(
                src_ref=ref,
                dst_ref=ref,
                send_sem=self.s,
                recv_sem=self.r.at[0],
                device_id=self.op,
                device_id_type=MESH,
            ).wait_send()

    def gathers(a, b, s, r):
        return (
            Gather(a, y, x, y_plus, y_minus, x_plus, x_minus, s.at[0], r.at[0]),
            Gather(b, x, y, x_plus, x_minus, y_plus, y_minus, s.at[1], r.at[1]),
        )

    crossings = ((0, 4), (-1, 8), (1, 12), (2, 16))

    def gather_start(pair):
        for g in pair:
            g.first()
        for g in pair:
            g.cross(0, 4)

    def gather_near(pair):
        for g in pair:
            g.near()
        for g in pair:
            g.cross(-1, 8)
            g.cross(1, 12)
        for g in pair:
            g.relay(0, 4)

    def gather_far(pair):
        for g in pair:
            g.far()
            g.cross(2, 16)
        for g in pair:
            g.relay(-1, 8)
            g.relay(1, 12)

    def gather_relays(pair):
        for g in pair:
            g.relay(2, 16)

    def gather_last(pair):
        for di, sem in crossings:
            for g in pair:
                g.last(di, sem)

    ones = jnp.ones((GROUP, COL), BF16)

    def features(is_a, group, j):
        return group * SIDE + j if is_a else j * SIDE + group

    def weight_rows(ref, is_a, group):
        if is_a:
            return ref[pl.ds(pl.multiple_of(group * GROUP, GROUP), GROUP), :]
        return jnp.concatenate(
            [
                ref[pl.ds(pl.multiple_of(features(False, group, j) * COL, COL), COL), :]
                for j in range(SIDE)
            ],
            axis=0,
        )

    def weight_columns(ref, is_a, group):
        if is_a:
            return ref[:, pl.ds(pl.multiple_of(group * GROUP, GROUP), GROUP)]
        return jnp.concatenate(
            [
                ref[:, pl.ds(pl.multiple_of(features(False, group, j) * COL, COL), COL)]
                for j in range(SIDE)
            ],
            axis=1,
        )

    def use_rows(buf, is_a, group, gain_at, outs, sq, start, at=0):
        h = buf.shape[1]
        scaled, squares = [], []
        for j in range(SIDE):
            part = buf[group * SIDE + j].astype(F32)
            scaled.append((part * gains[gain_at + features(is_a, group, j)]).astype(BF16))
            squares.append((part * part).astype(BF16))
        scaled, squares = jnp.concatenate(scaled, axis=1), jnp.concatenate(squares, axis=1)
        rows = pl.ds(at if is_a else at + h, h)
        found = [(sq, dot(squares, ones))]
        for ref, acc in outs:
            if ref.shape[0] > ref.shape[1]:
                found.append((acc, dot(scaled, weight_rows(ref, is_a, group))))
            else:
                found.append((acc, dot_t(scaled, weight_columns(ref, is_a, group))))
        for acc, got in found:
            acc[rows, :] = got if start else acc[rows, :] + got

    pieces = ((2,), (1, -1, 0))

    class Scatter:
        def __init__(self, p, o1, n1, o2, n2, outer, inner, op, om, ip, im, s, r, make):
            self.p, self.o1, self.n1, self.o2, self.n2 = p, o1, n1, o2, n2
            self.outer, self.inner = outer, inner
            self.op, self.om, self.ip, self.im = op, om, ip, im
            self.s, self.r, self.make = s, r, make
            self.h = p.shape[1]
            self.q = self.h // 2
            self.lo, self.hi = pl.ds(0, self.q), pl.ds(self.q, self.q)

        def copy(self, src, dst, sem, to):
            return pltpu.make_async_remote_copy(
                src_ref=src,
                dst_ref=dst,
                send_sem=self.s,
                recv_sem=self.r.at[sem],
                device_id=to,
                device_id_type=MESH,
            )

        def produce(self, do):
            group = on(self.outer, do)
            got = self.make(group)
            for j in range(SIDE):
                self.p[group * SIDE + j] = got[:, j * COL : (j + 1) * COL].astype(BF16)

        def row(self, do, di, rows):
            return self.p.at[on(self.outer, do) * SIDE + on(self.inner, di), rows]

        def outward(self, name, ds):
            do, rows, buf, slot, sem, to = {
                "a": (2, self.lo, self.o1, 0, 0, self.op),
                "b": (2, self.hi, self.o1, 1, 1, self.om),
                "c": (1, self.hi, self.n1, 0, 2, self.op),
                "d": (-1, self.lo, self.n1, 1, 3, self.om),
                "e": (1, self.lo, self.n1, 0, 4, self.op),
                "f": (-1, self.hi, self.n1, 1, 5, self.om),
            }[name]
            sem = sem if len(ds) == 1 else sem + 6
            whole_buf = buf is self.o1

            def target(place):
                return buf.at[slot, place] if whole_buf else buf.at[slot, place, rows]

            three = pl.ds(0, len(ds))
            pairs = [(self.row(do, di, rows), target(on(self.inner, di))) for di in ds]
            pairs.append((self.p.at[three, rows], target(three)))
            return [(src, dst, sem, to) for src, dst in pairs]

        def send(self, name, ds):
            for parts in self.outward(name, ds)[:-1]:
                self.copy(*parts).start()

        def wait(self, name, ds):
            self.copy(*self.outward(name, ds)[-1]).wait_recv()

        def leg2(self, name):
            di, rows, buf, slot, sem, to = {
                "a": (2, self.lo, self.o2, 0, 12, self.ip),
                "b": (2, self.hi, self.o2, 1, 13, self.im),
                "c": (1, self.hi, self.n2, 0, 14, self.ip),
                "d": (-1, self.lo, self.n2, 1, 15, self.im),
                "e": (1, self.lo, self.n2, 0, 16, self.ip),
                "f": (-1, self.hi, self.n2, 1, 17, self.im),
            }[name]
            dst = buf.at[slot] if buf is self.o2 else buf.at[slot, rows]
            return self.copy(self.row(0, di, rows), dst, sem, to)

        def start1(self):
            self.produce(2)
            for ds in pieces:
                self.send("a", ds)
                self.send("b", ds)

        def direct1(self):
            self.produce(1)
            for ds in pieces:
                self.send("c", ds)
            self.produce(-1)
            for ds in pieces:
                self.send("d", ds)

        def add(self, dst, src):
            dst[...] = (dst[...].astype(F32) + src[...].astype(F32)).astype(BF16)

        def relay1(self, ds):
            self.wait("a", ds)
            for di in ds:
                self.add(self.row(1, di, self.lo), self.o1.at[0, on(self.inner, di)])
            self.send("e", ds)
            self.wait("b", ds)
            for di in ds:
                self.add(self.row(-1, di, self.hi), self.o1.at[1, on(self.inner, di)])
            self.send("f", ds)

        def settle1(self, ds):
            for leg in "cdef":
                self.wait(leg, ds)
            for di in ds:
                place = on(self.inner, di)
                here = self.p.at[self.outer * SIDE + place]
                here[...] = (
                    here[...].astype(F32)
                    + self.n1[0, place].astype(F32)
                    + self.n1[1, place].astype(F32)
                ).astype(BF16)
                for leg in {2: "ab", 1: "c", -1: "d", 0: ""}[di]:
                    self.leg2(leg).start()

        def relay2(self):
            self.leg2("a").wait_recv()
            self.add(self.row(0, 1, self.lo), self.o2.at[0])
            self.leg2("e").start()
            self.leg2("b").wait_recv()
            self.add(self.row(0, -1, self.hi), self.o2.at[1])
            self.leg2("f").start()

        def settle2(self):
            for leg in "cdef":
                self.leg2(leg).wait_recv()
            mine = self.p[self.outer * SIDE + self.inner].astype(F32)
            return mine + self.n2[0].astype(F32) + self.n2[1].astype(F32)

        def drain(self):
            ref = self.p.at[pl.ds(0, SIDE * SIDE - 1)]
            self.copy(ref, ref, 0, self.op).wait_send()

    def scatters(left, w, pa, pb, oa, ob, na, nb, o2a, o2b, n2a, n2b, s, r):
        h = pa.shape[1]

        def make_a(group):
            return dot(left()[0:h], weight_columns(w, True, group))

        def make_b(group):
            return dot(left()[h : 2 * h], weight_columns(w, False, group))

        return (
            Scatter(
                pa, oa, na, o2a, n2a, y, x, y_plus, y_minus, x_plus, x_minus, s.at[0], r.at[0], make_a
            ),
            Scatter(
                pb, ob, nb, o2b, n2b, x, y, x_plus, x_minus, y_plus, y_minus, s.at[1], r.at[1], make_b
            ),
        )

    def scatter_start(pair):
        for g in pair:
            g.start1()
        for g in pair:
            g.direct1()

    def scatter_relay(pair, piece):
        for g in pair:
            g.relay1(pieces[piece])

    def scatter_own(pair):
        for g in pair:
            g.produce(0)

    def scatter_settle(pair, piece):
        for g in pair:
            g.settle1(pieces[piece])

    def scatter_relay2(pair):
        for g in pair:
            g.relay2()

    def scatter_end(pair):
        got = [g.settle2() for g in pair]
        for g in pair:
            g.drain()
        return got

    live = {}
    stores = [
        pltpu.make_async_copy(mix_out, mix_out_h, osem.at[0]),
        pltpu.make_async_copy(moe_out, moe_out_h, osem.at[1]),
    ]
    mix = gathers(xa, xb, agx_s, agx_r)
    xo = [(wm, acc_x)]

    def x_start():
        gather_start(mix)

    def x_near():
        gather_near(mix)

    def x_far():
        gather_far(mix)
        for load in loads:
            load.wait()
        use_rows(xa, True, y, 0, xo, sq_x, True)
        use_rows(xb, False, x, 0, xo, sq_x, True)

    def x_relays():
        gather_relays(mix)
        for d in (-1, 1):
            use_rows(xa, True, on(y, d), 0, xo, sq_x, False)
            use_rows(xb, False, on(x, d), 0, xo, sq_x, False)

    width = SIDE * SIDE * COL

    def x_last():
        gather_last(mix)
        use_rows(xa, True, on(y, 2), 0, xo, sq_x, False)
        use_rows(xb, False, on(x, 2), 0, xo, sq_x, False)
        for g in mix:
            g.drain()

    def recurrence():
        scale = lax.rsqrt(sq_x[...] * (1.0 / width) + epsilon)
        query = jax.nn.silu(acc_x[:, 0:COL] * scale)
        key = gap[...] * jax.nn.sigmoid(-(acc_x[:, COL : 2 * COL] * scale))
        value = (acc_x[:, 2 * COL : 3 * COL] * scale).astype(BF16)
        gate_out = jax.nn.silu(acc_x[:, 3 * COL : 4 * COL] * scale)
        extra = jnp.broadcast_to(decay[...], (COL, decay.shape[1])).T
        log_forget = jnp.log1p(-key) + extra
        part = half_x
        row = lax.broadcasted_iota(jnp.int32, (part, part), 0)
        col = lax.broadcasted_iota(jnp.int32, (part, part), 1)
        causal = row >= col
        lower = jnp.where(causal, 1.0, 0.0)
        outs, running, states, ends = [], [], [], []
        for c in range(2):
            rows = slice(c * part, (c + 1) * part)
            run = jnp.dot(lower, log_forget[rows], precision=HIGHEST, preferred_element_type=F32)
            mid, end = run[part // 2 - 1 : part // 2], run[part - 1 : part]
            q_in = (query[rows] * jnp.exp(run - mid)).astype(BF16)
            k_in = (key[rows] * jnp.exp(mid - run)).astype(BF16)
            near = lax.dot_general(q_in, k_in, (((1,), (1,)), ((), ())), preferred_element_type=F32)
            near = jnp.where(causal, near, 0.0).astype(BF16)
            outs.append(dot(near, value[rows]))
            k_end = (key[rows] * jnp.exp(end - run)).astype(BF16)
            states.append(
                lax.dot_general(value[rows], k_end, (((0,), (0,)), ((), ())), preferred_element_type=F32)
            )
            running.append(run)
            ends.append(end)
        q_second = (query[part:] * jnp.exp(running[1])).astype(BF16)
        outs[1] = outs[1] + lax.dot_general(
            q_second, states[0].astype(BF16), (((1,), (1,)), ((), ())), preferred_element_type=F32
        )
        state = states[0] * jnp.exp(ends[1]) + states[1]
        passing = jnp.exp(ends[0] + ends[1])
        q_enter = jnp.concatenate(
            [
                (query[:part] * jnp.exp(running[0])).astype(BF16),
                (query[part:] * jnp.exp(ends[0] + running[1])).astype(BF16),
            ],
            axis=0,
        )
        local_out = jnp.concatenate(outs, axis=0)
        st_out[...] = jnp.concatenate(
            [
                state.reshape(slices, 8, COL),
                jnp.broadcast_to(passing.reshape(1, 1, COL), (slices, 8, COL)),
            ],
            axis=1,
        ).astype(BF16)


        def to_owner(k, carry):
            peer = 2 * k + lax.rem(k, 2)

            @pl.when(peer != ep)
            def _():
                pltpu.make_async_remote_copy(
                    src_ref=st_out.at[k],
                    dst_ref=st_in.at[ep],
                    send_sem=a2a_s.at[2],
                    recv_sem=a2a_r.at[4],
                    device_id=(peer, tp),
                    device_id_type=MESH,
                ).start()

            return carry

        lax.fori_loop(0, slices, to_owner, 0)

        @pl.when(owner)
        def _():
            st_in[ep] = st_out[z]
        live.update(local_out=local_out, q_enter=q_enter, gate_out=gate_out)

    slices = COL // 8
    owner = core == lax.rem(z, 2)
    not_owner = jnp.logical_not(owner)

    def chain_states():
        @pl.when(owner)
        def _():
            whole(st_in, st_in, 2, n_ep - 1, 4).wait_recv()

            def chain(j, entering):
                block = st_in[j].astype(F32)
                st_back[j] = entering
                return block[8:16] * entering + block[0:8]

            lax.fori_loop(0, n_ep, chain, jnp.zeros((8, COL), F32))

            def give(o, carry):
                peer = lax.rem(ep + o, n_ep)
                pltpu.make_async_remote_copy(
                    src_ref=st_back.at[peer],
                    dst_ref=st_enter.at[z],
                    send_sem=a2a_s.at[3],
                    recv_sem=a2a_r.at[5],
                    device_id=(peer, tp),
                    device_id_type=MESH,
                ).start()
                return carry

            lax.fori_loop(1, n_ep, give, 0)
            st_enter[z] = st_back[ep]

    moe_gain_at = SIDE * SIDE
    half_m = ma.shape[2]
    chunks = []

    class Chunk:
        def __init__(self, c):
            self.c = c
            self.a, self.b = ma.at[c], mb.at[c]
            self.pair = gathers(self.a, self.b, agm_s.at[c], agm_r.at[c])
            self.at = 2 * half_m * c
            self.outs = [(wg, acc_g), (wu, acc_u)]

        def use(self, d, start):
            use_rows(self.a, True, on(y, d), moe_gain_at, self.outs, sq_m, start, self.at)
            use_rows(self.b, False, on(x, d), moe_gain_at, self.outs, sq_m, start, self.at)

        def start(self):
            whole(slots, arrived, 0, half_ep - (1 if self.c == 0 else 0), self.c).wait_recv()
            got = arrived[half_ep * self.c : half_ep * (self.c + 1)].astype(F32)
            got = got.reshape(2 * half_m, COL).astype(BF16)
            self.a[mine_a] = got[0:half_m]
            self.b[mine_b] = got[half_m:]
            gather_start(self.pair)

        def near(self):
            gather_near(self.pair)

        def far(self):
            gather_far(self.pair)
            self.use(0, True)

        def relays(self):
            gather_relays(self.pair)
            self.use(-1, False)
            self.use(1, False)

        def last(self):
            gather_last(self.pair)
            self.use(2, False)
            for g in self.pair:
                g.drain()

        def experts(self):
            rows = pl.ds(self.at, 2 * half_m)
            scale = lax.rsqrt(sq_m[rows, 0:1] * (1.0 / width) + epsilon)
            hidden = (jax.nn.silu(acc_g[rows, :] * scale) * (acc_u[rows, :] * scale)).astype(BF16)
            refs = [ref.at[self.c] for ref in (pma, pmb, oma, omb, nma, nmb, o2ma, o2mb, n2ma, n2mb)]
            self.sums = scatters(lambda: hidden, wd, *refs, rsm_s.at[self.c], rsm_r.at[self.c])

        def sum_start(self):
            for g in self.sums:
                g.start1()

        def sum_direct(self):
            for g in self.sums:
                g.direct1()

        def sum_relay(self, piece):
            scatter_relay(self.sums, piece)

        def sum_own(self):
            scatter_own(self.sums)

        def sum_settle(self, piece):
            scatter_settle(self.sums, piece)

        def sum_relay2(self):
            scatter_relay2(self.sums)

        def give_back(self):
            got = jnp.concatenate(scatter_end(self.sums), axis=0)
            first = half_ep * self.c
            outgoing[first : first + half_ep] = got.reshape(half_ep, cap, COL).astype(BF16)
            send_all(lambda i: return_copy(i, self.c), first, half_ep)
            if self.c == 0:
                returned[ep] = outgoing[own_place]

    near_chunk, far_chunk = Chunk(0), Chunk(1)

    def x_sum_start():
        @pl.when(owner)
        def _():
            whole(st_back, st_enter, 3, slices - 1, 5).wait_recv()

        @pl.when(not_owner)
        def _():
            whole(st_back, st_enter, 3, slices, 5).wait_recv()

        entering = st_enter[...].reshape(COL, COL).astype(BF16)
        head_out = live["local_out"] + lax.dot_general(
            live["q_enter"], entering, (((1,), (1,)), ((), ())), preferred_element_type=F32
        )
        mean = jnp.mean(head_out * head_out, axis=1, keepdims=True)
        gated = head_out * lax.rsqrt(mean + epsilon) * head_gain[...].astype(F32) * live["gate_out"]
        gated = gated.astype(BF16)
        refs = (pxa, pxb, oxa, oxb, nxa, nxb, o2xa, o2xb, n2xa, n2xb)
        live["sums"] = scatters(lambda: gated, wmix, *refs, rsx_s, rsx_r)
        scatter_start(live["sums"])

    def x_sum_relay(piece):
        scatter_relay(live["sums"], piece)

    def x_sum_own():
        scatter_own(live["sums"])

    def x_sum_settle(piece):
        scatter_settle(live["sums"], piece)

    def x_sum_relay2():
        scatter_relay2(live["sums"])

    def x_store():
        got = scatter_end(live["sums"])
        mix_out[0:half_x] = got[0].astype(BF16)
        mix_out[half_x : 2 * half_x] = got[1].astype(BF16)
        stores[0].start()

    def weigh():
        score0, score1 = places[:, 2:3], places[:, 3:4]
        total = score0 + score1
        slot = lax.broadcasted_iota(jnp.int32, (tok, n_ep * cap), 1).astype(F32)
        weight = jnp.where(slot == places[:, 0:1], score0 / total, 0.0)
        weight = weight + jnp.where(slot == places[:, 1:2], score1 / total, 0.0)
        coarse = weight.astype(BF16)
        fine = (weight - coarse.astype(F32)).astype(BF16)
        live.update(coarse=coarse, fine=fine)

    def combine():
        whole(outgoing, returned, 1, half_ep - 1, 2).wait_recv()
        whole(outgoing, returned, 1, half_ep, 3).wait_recv()
        results = returned[...].astype(F32).reshape(n_ep * cap, COL).astype(BF16)
        moe_out[...] = (dot(live["coarse"], results) + dot(live["fine"], results)).astype(BF16)
        stores[1].start()

    send_all(dispatch_copy, 0, half_ep)
    x_start()
    arrived[own_place] = slots[ep]
    x_near()
    send_all(dispatch_copy, half_ep, half_ep)
    near_chunk.start()
    x_far()
    near_chunk.near()
    x_relays()
    near_chunk.far()
    far_chunk.start()
    x_last()
    near_chunk.relays()
    far_chunk.near()
    recurrence()
    near_chunk.last()
    far_chunk.far()
    near_chunk.experts()
    near_chunk.sum_start()
    far_chunk.relays()
    near_chunk.sum_direct()
    near_chunk.sum_own()
    far_chunk.last()
    far_chunk.experts()
    far_chunk.sum_start()
    far_chunk.sum_direct()
    chain_states()
    far_chunk.sum_relay(0)
    far_chunk.sum_relay(1)
    far_chunk.sum_own()
    near_chunk.sum_relay(0)
    near_chunk.sum_relay(1)
    far_chunk.sum_settle(0)
    far_chunk.sum_settle(1)
    near_chunk.sum_settle(0)
    far_chunk.sum_relay2()
    near_chunk.sum_settle(1)
    x_sum_start()
    far_chunk.give_back()
    near_chunk.sum_relay2()
    x_sum_relay(0)
    x_sum_relay(1)
    near_chunk.give_back()
    x_sum_own()
    x_sum_settle(0)
    x_sum_settle(1)
    x_sum_relay2()
    weigh()
    x_store()
    combine()

    whole(slots, arrived, 0, n_ep - 1).wait_send()
    whole(outgoing, returned, 1, n_ep - 1).wait_send()

    @pl.when(owner)
    def _():
        whole(st_out, st_in, 2, slices - 1).wait_send()
        whole(st_back, st_back, 3, n_ep - 1).wait_send()

    @pl.when(not_owner)
    def _():
        whole(st_out, st_in, 2, slices).wait_send()

    for store in stores:
        store.wait()


def per_device(n_ep, *args):
    (
        mix_rows,
        mix_gain,
        w_query,
        w_forget,
        w_input,
        w_outgate,
        forget_gap,
        decay_extra,
        head_gain,
        w_mixout,
        moe_rows,
        moe_gain,
        route_ids,
        route_scores,
        w_gate,
        w_up,
        w_down,
    ) = args
    tok_a, tok_b = mix_rows.shape[0], moe_rows.shape[0]
    cap = tok_b * route_ids.shape[1] * 3 // (2 * n_ep)
    rows = n_ep * cap
    hidden = w_gate.shape[2]
    width = w_query.shape[0]
    hx, hm = tok_a // 2, rows // 4
    n_tp = SIDE * SIDE
    slices = COL // 8
    hbm = pl.BlockSpec(memory_space=pltpu.HBM)
    dma = pltpu.SemaphoreType.DMA

    def v(shape, dtype=BF16):
        return pltpu.VMEM(shape, dtype)

    def scatter_buffers(h, n=()):
        return [
            v((*n, n_tp, h, COL)),
            v((*n, n_tp, h, COL)),
            v((*n, 2, SIDE, h // 2, COL)),
            v((*n, 2, SIDE, h // 2, COL)),
            v((*n, 2, SIDE, h, COL)),
            v((*n, 2, SIDE, h, COL)),
        ]

    def scatter_ends(h, n=()):
        return [v((*n, 2, h // 2, COL)), v((*n, 2, h // 2, COL)), v((*n, 2, h, COL)), v((*n, 2, h, COL))]

    scratch = [
        v((tok_a, COL)),
        v((tok_b, COL)),
        v((n_tp, COL)),
        v((n_tp, COL)),
        v((1, COL), F32),
        v((1, tok_a), F32),
        v((1, COL)),
        v((2, tok_b), jnp.int32),
        v((2, tok_b), F32),
        v((tok_a, COL)),
        v((tok_b, COL)),
        v((width, 4 * COL)),
        v((COL, width)),
        v((hidden, width)),
        v((hidden, width)),
        v((hidden, width)),
        v((n_ep, cap, COL)),
        v((n_ep, cap, COL)),
        v((n_ep, cap, COL)),
        v((n_ep, cap, COL)),
        v((tok_b, COL), F32),
        v((2 * n_tp, 1, COL), F32),
        v((n_tp, hx, COL)),
        v((n_tp, hx, COL)),
        v((2, n_tp, hm, COL)),
        v((2, n_tp, hm, COL)),
        v((tok_a, 4 * COL), F32),
        v((tok_a, COL), F32),
        v((rows, hidden), F32),
        v((rows, hidden), F32),
        v((rows, COL), F32),
        v((slices, 16, COL)),
        v((n_ep, 16, COL)),
        v((n_ep, 8, COL), F32),
        v((slices, 8, COL), F32),
        *scatter_buffers(hx),
        *scatter_buffers(hm, (2,)),
        *scatter_ends(hx),
        *scatter_ends(hm, (2,)),
        dma((9,)),
        dma((2,)),
        dma((8,)),
        dma((4,)),
        dma((6,)),
        dma((2,)),
        dma((2, 20)),
        dma((2, 2)),
        dma((2, 2, 20)),
        dma((2,)),
        dma((2, 18)),
        dma((2, 2)),
        dma((2, 2, 18)),
    ]
    return pl.pallas_call(
        functools.partial(step_kernel, n_ep, cap),
        out_shape=[
            jax.ShapeDtypeStruct((tok_a, COL), BF16),
            jax.ShapeDtypeStruct((tok_b, COL), BF16),
        ],
        in_specs=[hbm] * 17,
        out_specs=[hbm, hbm],
        scratch_shapes=scratch,
        compiler_params=pltpu.CompilerParams(
            collective_id=0, has_side_effects=True, vmem_limit_bytes=63 * 1024 * 1024
        ),
    )(
        mix_rows,
        moe_rows,
        mix_gain.reshape(-1, COL),
        moe_gain.reshape(-1, COL),
        forget_gap.reshape(1, COL),
        decay_extra,
        head_gain.reshape(1, COL),
        route_ids.T,
        route_scores.T,
        w_query,
        w_forget,
        w_input,
        w_outgate,
        w_mixout,
        jnp.swapaxes(w_gate, 1, 2),
        jnp.swapaxes(w_up, 1, 2),
        w_down,
    )


def solution(mesh):
    placed = (
        P("ep", "tp"),
        P(),
        P(None, "tp"),
        P(None, "tp"),
        P(None, "tp"),
        P(None, "tp"),
        P("tp"),
        P("tp", "ep"),
        P(),
        P("tp", None),
        P("ep", "tp"),
        P(),
        P("ep", None),
        P("ep", None),
        P("ep", None, "tp"),
        P("ep", None, "tp"),
        P("ep", "tp", None),
    )
    return jax.shard_map(
        functools.partial(per_device, mesh.shape["ep"]),
        mesh=mesh,
        in_specs=placed,
        out_specs=(P("ep", "tp"), P("ep", "tp")),
        check_vma=False,
    )
```

```python
import functools

import jax
import jax.numpy as jnp
from jax import lax
from jax.experimental import pallas as pl
from jax.experimental.pallas import tpu as pltpu
from jax.sharding import PartitionSpec as P

MESH = pl.DeviceIdType.MESH
epsilon = 1e-06
HIGHEST = lax.Precision.HIGHEST
F32, BF16 = jnp.float32, jnp.bfloat16
SIDE = 4
COL = 128
GROUP = SIDE * COL


def dot(a, b):
    return jnp.dot(a, b, preferred_element_type=F32)


def dot_t(a, b):
    return lax.dot_general(a, b, (((1,), (1,)), ((), ())), preferred_element_type=F32)


def step_kernel(
    n_ep,
    cap,
    mix_rows_h,
    moe_rows_h,
    mix_gain_h,
    moe_gain_h,
    gap_h,
    decay_h,
    head_gain_h,
    ids_h,
    scores_h,
    wq_h,
    wf_h,
    wi_h,
    wo_h,
    wmix_h,
    wg_h,
    wu_h,
    wd_h,
    mix_out,
    moe_out,
    mix_rows,
    moe_rows,
    mix_gain,
    moe_gain,
    gap,
    decay,
    head_gain,
    ids,
    scores,
    wm,
    wmix,
    wg,
    wu,
    wd,
    slots,
    arrived,
    outgoing,
    returned,
    places,
    gains,
    xa,
    xb,
    ma,
    mb,
    acc_x,
    sq_x,
    acc_g,
    acc_u,
    sq_m,
    st_out,
    st_in,
    st_back,
    st_enter,
    pxa,
    pxb,
    oxa,
    oxb,
    nxa,
    nxb,
    pma,
    pmb,
    oma,
    omb,
    nma,
    nmb,
    o2xa,
    o2xb,
    n2xa,
    n2xb,
    o2ma,
    o2mb,
    n2ma,
    n2mb,
    isem,
    wsem,
    a2a_s,
    a2a_r,
    agx_s,
    agx_r,
    agm_s,
    agm_r,
    rsx_s,
    rsx_r,
    rsm_s,
    rsm_r,
):
    n_z = n_ep // 2
    ep = lax.axis_index("ep")
    tp = lax.axis_index("tp")
    x, y = lax.rem(tp, SIDE), tp // SIDE
    z, core = ep // 2, lax.rem(ep, 2)

    def on(v, d):
        return lax.rem(v + d + SIDE, SIDE)

    x_plus, x_minus = (ep, y * SIDE + on(x, 1)), (ep, y * SIDE + on(x, -1))
    y_plus, y_minus = (ep, on(y, 1) * SIDE + x), (ep, on(y, -1) * SIDE + x)

    firsts = [
        pltpu.make_async_copy(src, dst, isem.at[i])
        for i, (src, dst) in enumerate(
            [
                (ids_h, ids),
                (scores_h, scores),
                (moe_rows_h, moe_rows),
                (mix_rows_h, mix_rows),
                (mix_gain_h, mix_gain),
                (moe_gain_h, moe_gain),
                (gap_h, gap),
                (decay_h, decay),
                (head_gain_h, head_gain),
            ]
        )
    ]
    for first in firsts:
        first.start()
    loads = [
        pltpu.make_async_copy(src, dst, wsem.at[i])
        for i, (src, dst) in enumerate(
            [
                (wq_h, wm.at[:, 0:COL]),
                (wf_h, wm.at[:, COL : 2 * COL]),
                (wi_h, wm.at[:, 2 * COL : 3 * COL]),
                (wo_h, wm.at[:, 3 * COL : 4 * COL]),
                (wg_h.at[0], wg),
                (wu_h.at[0], wu),
                (wd_h.at[0], wd),
                (wmix_h, wmix),
            ]
        )
    ]
    barrier = pltpu.get_barrier_semaphore()
    for peer in (x_plus, x_minus, y_plus, y_minus):
        pl.semaphore_signal(barrier, inc=1, device_id=peer, device_id_type=MESH)

    def greet(o, carry):
        pl.semaphore_signal(
            barrier, inc=1, device_id=(lax.rem(ep + o, n_ep), tp), device_id_type=MESH
        )
        return carry

    lax.fori_loop(1, n_ep, greet, 0)

    for first in firsts:
        first.wait()
    for load in loads:
        load.start()


    gains[0 : SIDE * SIDE] = mix_gain[...].astype(F32).reshape(SIDE * SIDE, 1, COL)
    gains[SIDE * SIDE :] = moe_gain[...].astype(F32).reshape(SIDE * SIDE, 1, COL)

    tok = ids.shape[1]
    id0, id1 = ids[0:1], ids[1:2]
    expert = lax.broadcasted_iota(jnp.int32, (n_ep, tok), 0)
    one0, one1 = expert == id0, expert == id1
    named = jnp.where(one0 | one1, 1.0, 0.0).astype(BF16)
    row = lax.broadcasted_iota(jnp.int32, (tok, tok), 0)
    col = lax.broadcasted_iota(jnp.int32, (tok, tok), 1)
    before = jnp.where(row < col, 1.0, 0.0).astype(BF16)
    rank = dot(named, before)
    place0 = id0.astype(F32) * cap + jnp.sum(jnp.where(one0, rank, 0.0), axis=0, keepdims=True)
    place1 = id1.astype(F32) * cap + jnp.sum(jnp.where(one1, rank, 0.0), axis=0, keepdims=True)
    line = lax.broadcasted_iota(jnp.int32, (COL, tok), 0)
    table = jnp.where(line == 0, place0, place1)
    table = jnp.where(line == 2, scores[0:1], jnp.where(line == 3, scores[1:2], table))
    places[...] = table.T
    slot = lax.broadcasted_iota(jnp.int32, (n_ep * cap, tok), 0).astype(F32)
    pick = jnp.where((slot == place0) | (slot == place1), 1.0, 0.0).astype(BF16)
    slots[...] = dot(pick, moe_rows[...]).reshape(n_ep, cap, COL).astype(BF16)

    half_x = xa.shape[1]
    mine_a, mine_b = y * SIDE + x, x * SIDE + y
    xa[mine_a] = mix_rows[0:half_x]
    xb[mine_b] = mix_rows[half_x : 2 * half_x]

    pl.semaphore_wait(barrier, n_ep - 1 + 4)

    near_z = n_z // 4 - 1

    def partner(u, c, away):
        dz = u - near_z
        return 2 * lax.rem(z + (dz if away else -dz) + 2 * n_z, n_z) + c

    half_ep = n_ep // 2

    def dispatch_copy(i):
        u, c = i // 2, i % 2
        peer = partner(u, c, False)
        return pltpu.make_async_remote_copy(
            src_ref=slots.at[peer],
            dst_ref=arrived.at[2 * u + core],
            send_sem=a2a_s.at[0],
            recv_sem=a2a_r.at[i // half_ep],
            device_id=(peer, tp),
            device_id_type=MESH,
        )

    def return_copy(i, chunk):
        u, c = i // 2, i % 2
        peer = partner(u, c, True)
        return pltpu.make_async_remote_copy(
            src_ref=outgoing.at[i],
            dst_ref=returned.at[ep],
            send_sem=a2a_s.at[1],
            recv_sem=a2a_r.at[2 + chunk],
            device_id=(peer, tp),
            device_id_type=MESH,
        )

    own_place = 2 * near_z + core

    def send_all(make, chunk):
        half_z = n_z // 2
        ways = range(half_z * chunk, half_z * (chunk + 1))

        def far(u):
            ahead = (u - near_z) % n_z
            return -min(ahead, n_z - ahead)

        for u in sorted(ways, key=far):
            for c in range(2):
                copy = make(2 * u + c)
                if u != near_z:
                    copy.start()
                else:

                    @pl.when(core != c)
                    def _():
                        copy.start()

    def whole(src, dst, k, count, r=None):
        return pltpu.make_async_remote_copy(
            src_ref=src.at[pl.ds(0, count)],
            dst_ref=dst.at[pl.ds(0, count)],
            send_sem=a2a_s.at[k],
            recv_sem=a2a_r.at[k if r is None else r],
            device_id=(lax.rem(ep + 1, n_ep), tp),
            device_id_type=MESH,
        )

    class Gather:
        def __init__(self, buf, outer, inner, out_plus, out_minus, in_plus, in_minus, s, r):
            self.buf, self.outer, self.inner = buf, outer, inner
            self.op, self.om, self.ip, self.im = out_plus, out_minus, in_plus, in_minus
            self.s, self.r = s, r
            self.h = buf.shape[1]

        def at(self, do, di):
            return on(self.outer, do) * SIDE + on(self.inner, di)

        def copy(self, block, rows, sem, to):
            ref = self.buf.at[block] if rows is None else self.buf.at[block, pl.ds(*rows)]
            return pltpu.make_async_remote_copy(
                src_ref=ref,
                dst_ref=ref,
                send_sem=self.s,
                recv_sem=self.r.at[sem],
                device_id=to,
                device_id_type=MESH,
            )

        def first(self):
            q = self.h // 2
            self.lo, self.hi = (0, q), (q, q)
            self.copy(self.at(0, 0), None, 0, self.ip).start()
            self.copy(self.at(0, 0), None, 1, self.im).start()

        def cross(self, di, sem):
            self.copy(self.at(0, di), None, sem, self.op).start()
            self.copy(self.at(0, di), None, sem + 1, self.om).start()

        def near(self):
            self.copy(self.at(0, -1), None, 0, self.ip).wait_recv()
            self.copy(self.at(0, -1), self.lo, 2, self.ip).start()
            self.copy(self.at(0, 1), None, 1, self.im).wait_recv()
            self.copy(self.at(0, 1), self.hi, 3, self.im).start()

        def far(self):
            self.copy(self.at(0, 2), self.lo, 2, self.ip).wait_recv()
            self.copy(self.at(0, 2), self.hi, 3, self.im).wait_recv()

        def relay(self, di, sem):
            self.copy(self.at(-1, di), None, sem, self.op).wait_recv()
            self.copy(self.at(-1, di), self.lo, sem + 2, self.op).start()
            self.copy(self.at(1, di), None, sem + 1, self.om).wait_recv()
            self.copy(self.at(1, di), self.hi, sem + 3, self.om).start()

        def last(self, di, sem):
            self.copy(self.at(2, di), self.lo, sem + 2, self.op).wait_recv()
            self.copy(self.at(2, di), self.hi, sem + 3, self.om).wait_recv()

        def drain(self):
            ref = self.buf.at[pl.ds(0, SIDE * SIDE - 1)]
            pltpu.make_async_remote_copy(
                src_ref=ref,
                dst_ref=ref,
                send_sem=self.s,
                recv_sem=self.r.at[0],
                device_id=self.op,
                device_id_type=MESH,
            ).wait_send()

    def gathers(a, b, s, r):
        return (
            Gather(a, y, x, y_plus, y_minus, x_plus, x_minus, s.at[0], r.at[0]),
            Gather(b, x, y, x_plus, x_minus, y_plus, y_minus, s.at[1], r.at[1]),
        )

    crossings = ((0, 4), (-1, 8), (1, 12), (2, 16))

    def gather_start(pair):
        for g in pair:
            g.first()
        for g in pair:
            g.cross(0, 4)

    def gather_near_a(pair):
        for g in pair:
            g.near()
        for g in pair:
            g.cross(-1, 8)
            g.cross(1, 12)

    def gather_near_b(pair):
        for g in pair:
            g.relay(0, 4)

    def gather_near(pair):
        gather_near_a(pair)
        gather_near_b(pair)

    def gather_far(pair):
        for g in pair:
            g.far()
            g.cross(2, 16)
        for g in pair:
            g.relay(-1, 8)
            g.relay(1, 12)

    def gather_relays(pair):
        for g in pair:
            g.relay(2, 16)

    def gather_last(pair):
        for di, sem in crossings:
            for g in pair:
                g.last(di, sem)

    ones = jnp.ones((GROUP, COL), BF16)

    def features(is_a, group, j):
        return group * SIDE + j if is_a else j * SIDE + group

    def weight_rows(ref, is_a, group):
        if is_a:
            return ref[pl.ds(pl.multiple_of(group * GROUP, GROUP), GROUP), :]
        return jnp.concatenate(
            [
                ref[pl.ds(pl.multiple_of(features(False, group, j) * COL, COL), COL), :]
                for j in range(SIDE)
            ],
            axis=0,
        )

    def weight_columns(ref, is_a, group):
        if is_a:
            return ref[:, pl.ds(pl.multiple_of(group * GROUP, GROUP), GROUP)]
        return jnp.concatenate(
            [
                ref[:, pl.ds(pl.multiple_of(features(False, group, j) * COL, COL), COL)]
                for j in range(SIDE)
            ],
            axis=1,
        )

    def use_rows(buf, is_a, group, gain_at, outs, sq, start, at=0):
        h = buf.shape[1]
        scaled, squares = [], []
        for j in range(SIDE):
            part = buf[group * SIDE + j].astype(F32)
            scaled.append((part * gains[gain_at + features(is_a, group, j)]).astype(BF16))
            squares.append((part * part).astype(BF16))
        scaled, squares = jnp.concatenate(scaled, axis=1), jnp.concatenate(squares, axis=1)
        rows = pl.ds(at if is_a else at + h, h)
        found = [(sq, dot(squares, ones))]
        for ref, acc in outs:
            if ref.shape[0] > ref.shape[1]:
                found.append((acc, dot(scaled, weight_rows(ref, is_a, group))))
            else:
                found.append((acc, dot_t(scaled, weight_columns(ref, is_a, group))))
        for acc, got in found:
            acc[rows, :] = got if start else acc[rows, :] + got

    pieces = ((2,), (1, -1, 0))

    class Scatter:
        def __init__(self, p, o1, n1, o2, n2, outer, inner, op, om, ip, im, s, r, make):
            self.p, self.o1, self.n1, self.o2, self.n2 = p, o1, n1, o2, n2
            self.outer, self.inner = outer, inner
            self.op, self.om, self.ip, self.im = op, om, ip, im
            self.s, self.r, self.make = s, r, make
            self.h = p.shape[1]
            self.q = self.h // 2
            self.lo, self.hi = pl.ds(0, self.q), pl.ds(self.q, self.q)

        def copy(self, src, dst, sem, to):
            return pltpu.make_async_remote_copy(
                src_ref=src,
                dst_ref=dst,
                send_sem=self.s,
                recv_sem=self.r.at[sem],
                device_id=to,
                device_id_type=MESH,
            )

        def produce(self, do):
            group = on(self.outer, do)
            got = self.make(group)
            for j in range(SIDE):
                self.p[group * SIDE + j] = got[:, j * COL : (j + 1) * COL].astype(BF16)

        def row(self, do, di, rows):
            return self.p.at[on(self.outer, do) * SIDE + on(self.inner, di), rows]

        def outward(self, name, ds):
            do, rows, buf, slot, sem, to = {
                "a": (2, self.lo, self.o1, 0, 0, self.op),
                "b": (2, self.hi, self.o1, 1, 1, self.om),
                "c": (1, self.hi, self.n1, 0, 2, self.op),
                "d": (-1, self.lo, self.n1, 1, 3, self.om),
                "e": (1, self.lo, self.n1, 0, 4, self.op),
                "f": (-1, self.hi, self.n1, 1, 5, self.om),
            }[name]
            sem = sem if len(ds) == 1 else sem + 6
            whole_buf = buf is self.o1

            def target(place):
                return buf.at[slot, place] if whole_buf else buf.at[slot, place, rows]

            three = pl.ds(0, len(ds))
            pairs = [(self.row(do, di, rows), target(on(self.inner, di))) for di in ds]
            pairs.append((self.p.at[three, rows], target(three)))
            return [(src, dst, sem, to) for src, dst in pairs]

        def send(self, name, ds):
            for parts in self.outward(name, ds)[:-1]:
                self.copy(*parts).start()

        def wait(self, name, ds):
            self.copy(*self.outward(name, ds)[-1]).wait_recv()

        def leg2(self, name):
            di, rows, buf, slot, sem, to = {
                "a": (2, self.lo, self.o2, 0, 12, self.ip),
                "b": (2, self.hi, self.o2, 1, 13, self.im),
                "c": (1, self.hi, self.n2, 0, 14, self.ip),
                "d": (-1, self.lo, self.n2, 1, 15, self.im),
                "e": (1, self.lo, self.n2, 0, 16, self.ip),
                "f": (-1, self.hi, self.n2, 1, 17, self.im),
            }[name]
            dst = buf.at[slot] if buf is self.o2 else buf.at[slot, rows]
            return self.copy(self.row(0, di, rows), dst, sem, to)

        def start1(self):
            self.produce(2)
            for ds in pieces:
                self.send("a", ds)
                self.send("b", ds)

        def direct1(self):
            self.produce(1)
            for ds in pieces:
                self.send("c", ds)
            self.produce(-1)
            for ds in pieces:
                self.send("d", ds)

        def add(self, dst, src):
            dst[...] = (dst[...].astype(F32) + src[...].astype(F32)).astype(BF16)

        def relay1(self, ds):
            self.wait("a", ds)
            for di in ds:
                self.add(self.row(1, di, self.lo), self.o1.at[0, on(self.inner, di)])
            self.send("e", ds)
            self.wait("b", ds)
            for di in ds:
                self.add(self.row(-1, di, self.hi), self.o1.at[1, on(self.inner, di)])
            self.send("f", ds)

        def settle1(self, ds):
            for leg in "cdef":
                self.wait(leg, ds)
            for di in ds:
                place = on(self.inner, di)
                here = self.p.at[self.outer * SIDE + place]
                here[...] = (
                    here[...].astype(F32)
                    + self.n1[0, place].astype(F32)
                    + self.n1[1, place].astype(F32)
                ).astype(BF16)
                for leg in {2: "ab", 1: "c", -1: "d", 0: ""}[di]:
                    self.leg2(leg).start()

        def relay2(self):
            self.leg2("a").wait_recv()
            self.add(self.row(0, 1, self.lo), self.o2.at[0])
            self.leg2("e").start()
            self.leg2("b").wait_recv()
            self.add(self.row(0, -1, self.hi), self.o2.at[1])
            self.leg2("f").start()

        def settle2(self):
            for leg in "cdef":
                self.leg2(leg).wait_recv()
            mine = self.p[self.outer * SIDE + self.inner].astype(F32)
            return mine + self.n2[0].astype(F32) + self.n2[1].astype(F32)

        def drain(self):
            ref = self.p.at[pl.ds(0, SIDE * SIDE - 1)]
            self.copy(ref, ref, 0, self.op).wait_send()

    def scatters(left, w, pa, pb, oa, ob, na, nb, o2a, o2b, n2a, n2b, s, r):
        h = pa.shape[1]

        def make_a(group):
            return dot(left()[0:h], weight_columns(w, True, group))

        def make_b(group):
            return dot(left()[h : 2 * h], weight_columns(w, False, group))

        return (
            Scatter(
                pa, oa, na, o2a, n2a, y, x, y_plus, y_minus, x_plus, x_minus, s.at[0], r.at[0], make_a
            ),
            Scatter(
                pb, ob, nb, o2b, n2b, x, y, x_plus, x_minus, y_plus, y_minus, s.at[1], r.at[1], make_b
            ),
        )

    def scatter_start(pair):
        for g in pair:
            g.start1()
        for g in pair:
            g.direct1()

    def scatter_relay(pair, piece):
        for g in pair:
            g.relay1(pieces[piece])

    def scatter_own(pair):
        for g in pair:
            g.produce(0)

    def scatter_settle(pair, piece):
        for g in pair:
            g.settle1(pieces[piece])

    def scatter_relay2(pair):
        for g in pair:
            g.relay2()

    def scatter_end(pair):
        got = [g.settle2() for g in pair]
        for g in pair:
            g.drain()
        return got

    live = {}
    mix = gathers(xa, xb, agx_s, agx_r)
    xo = [(wm, acc_x)]

    def x_start():
        gather_start(mix)

    def x_near():
        gather_near(mix)

    def x_near_a():
        gather_near_a(mix)

    def x_near_b():
        gather_near_b(mix)

    def x_far():
        gather_far(mix)
        for load in loads:
            load.wait()
        use_rows(xa, True, y, 0, xo, sq_x, True)
        use_rows(xb, False, x, 0, xo, sq_x, True)

    def x_relays():
        gather_relays(mix)
        for d in (-1, 1):
            use_rows(xa, True, on(y, d), 0, xo, sq_x, False)
            use_rows(xb, False, on(x, d), 0, xo, sq_x, False)

    width = SIDE * SIDE * COL

    def x_last():
        gather_last(mix)
        use_rows(xa, True, on(y, 2), 0, xo, sq_x, False)
        use_rows(xb, False, on(x, 2), 0, xo, sq_x, False)
        for g in mix:
            g.drain()

    def recurrence():
        scale = lax.rsqrt(sq_x[...] * (1.0 / width) + epsilon)
        query = jax.nn.silu(acc_x[:, 0:COL] * scale)
        key = gap[...] * jax.nn.sigmoid(-(acc_x[:, COL : 2 * COL] * scale))
        value = (acc_x[:, 2 * COL : 3 * COL] * scale).astype(BF16)
        gate_out = jax.nn.silu(acc_x[:, 3 * COL : 4 * COL] * scale)
        extra = jnp.broadcast_to(decay[...], (COL, decay.shape[1])).T
        log_forget = jnp.log1p(-key) + extra
        part = half_x
        row = lax.broadcasted_iota(jnp.int32, (part, part), 0)
        col = lax.broadcasted_iota(jnp.int32, (part, part), 1)
        causal = row >= col
        lower = jnp.where(causal, 1.0, 0.0)
        outs, running, states, ends = [], [], [], []
        for c in range(2):
            rows = slice(c * part, (c + 1) * part)
            run = jnp.dot(lower, log_forget[rows], precision=HIGHEST, preferred_element_type=F32)
            mid, end = run[part // 2 - 1 : part // 2], run[part - 1 : part]
            q_in = (query[rows] * jnp.exp(run - mid)).astype(BF16)
            k_in = (key[rows] * jnp.exp(mid - run)).astype(BF16)
            near = lax.dot_general(q_in, k_in, (((1,), (1,)), ((), ())), preferred_element_type=F32)
            near = jnp.where(causal, near, 0.0).astype(BF16)
            outs.append(dot(near, value[rows]))
            k_end = (key[rows] * jnp.exp(end - run)).astype(BF16)
            states.append(
                lax.dot_general(value[rows], k_end, (((0,), (0,)), ((), ())), preferred_element_type=F32)
            )
            running.append(run)
            ends.append(end)
        q_second = (query[part:] * jnp.exp(running[1])).astype(BF16)
        outs[1] = outs[1] + lax.dot_general(
            q_second, states[0].astype(BF16), (((1,), (1,)), ((), ())), preferred_element_type=F32
        )
        state = states[0] * jnp.exp(ends[1]) + states[1]
        passing = jnp.exp(ends[0] + ends[1])
        q_enter = jnp.concatenate(
            [
                (query[:part] * jnp.exp(running[0])).astype(BF16),
                (query[part:] * jnp.exp(ends[0] + running[1])).astype(BF16),
            ],
            axis=0,
        )
        local_out = jnp.concatenate(outs, axis=0)
        st_out[...] = jnp.concatenate(
            [
                state.reshape(slices, 8, COL),
                jnp.broadcast_to(passing.reshape(1, 1, COL), (slices, 8, COL)),
            ],
            axis=1,
        ).astype(BF16)


        def to_owner(k, carry):
            peer = 2 * k + lax.rem(k, 2)

            @pl.when(peer != ep)
            def _():
                pltpu.make_async_remote_copy(
                    src_ref=st_out.at[k],
                    dst_ref=st_in.at[ep],
                    send_sem=a2a_s.at[2],
                    recv_sem=a2a_r.at[4],
                    device_id=(peer, tp),
                    device_id_type=MESH,
                ).start()

            return carry

        lax.fori_loop(0, slices, to_owner, 0)

        @pl.when(owner)
        def _():
            st_in[ep] = st_out[z]
        live.update(local_out=local_out, q_enter=q_enter, gate_out=gate_out)

    slices = COL // 8
    owner = core == lax.rem(z, 2)
    not_owner = jnp.logical_not(owner)

    def chain_states():
        @pl.when(owner)
        def _():
            whole(st_in, st_in, 2, n_ep - 1, 4).wait_recv()

            def chain(j, entering):
                block = st_in[j].astype(F32)
                st_back[j] = entering
                return block[8:16] * entering + block[0:8]

            lax.fori_loop(0, n_ep, chain, jnp.zeros((8, COL), F32))

            def give(o, carry):
                peer = lax.rem(ep + o, n_ep)
                pltpu.make_async_remote_copy(
                    src_ref=st_back.at[peer],
                    dst_ref=st_enter.at[z],
                    send_sem=a2a_s.at[3],
                    recv_sem=a2a_r.at[5],
                    device_id=(peer, tp),
                    device_id_type=MESH,
                ).start()
                return carry

            lax.fori_loop(1, n_ep, give, 0)
            st_enter[z] = st_back[ep]

    moe_gain_at = SIDE * SIDE
    half_m = ma.shape[2]
    chunks = []

    class Chunk:
        def __init__(self, c):
            self.c = c
            self.a, self.b = ma.at[c], mb.at[c]
            self.pair = gathers(self.a, self.b, agm_s.at[c], agm_r.at[c])
            self.at = 2 * half_m * c
            self.outs = [(wg, acc_g), (wu, acc_u)]

        def use(self, d, start):
            use_rows(self.a, True, on(y, d), moe_gain_at, self.outs, sq_m, start, self.at)
            use_rows(self.b, False, on(x, d), moe_gain_at, self.outs, sq_m, start, self.at)

        def start(self):
            whole(slots, arrived, 0, half_ep - (1 if self.c == 0 else 0), self.c).wait_recv()
            got = arrived[half_ep * self.c : half_ep * (self.c + 1)].astype(F32)
            got = got.reshape(2 * half_m, COL).astype(BF16)
            self.a[mine_a] = got[0:half_m]
            self.b[mine_b] = got[half_m:]
            gather_start(self.pair)

        def near(self):
            gather_near(self.pair)

        def far(self):
            gather_far(self.pair)
            self.use(0, True)

        def relays(self):
            gather_relays(self.pair)
            self.use(-1, False)
            self.use(1, False)

        def last(self):
            gather_last(self.pair)
            self.use(2, False)
            for g in self.pair:
                g.drain()

        def experts(self):
            rows = pl.ds(self.at, 2 * half_m)
            scale = lax.rsqrt(sq_m[rows, 0:1] * (1.0 / width) + epsilon)
            hidden = (jax.nn.silu(acc_g[rows, :] * scale) * (acc_u[rows, :] * scale)).astype(BF16)
            refs = [ref.at[self.c] for ref in (pma, pmb, oma, omb, nma, nmb, o2ma, o2mb, n2ma, n2mb)]
            self.sums = scatters(lambda: hidden, wd, *refs, rsm_s.at[self.c], rsm_r.at[self.c])

        def sum_start(self):
            for g in self.sums:
                g.start1()

        def sum_direct(self):
            for g in self.sums:
                g.direct1()

        def sum_relay(self, piece):
            scatter_relay(self.sums, piece)

        def sum_own(self):
            scatter_own(self.sums)

        def sum_settle(self, piece):
            scatter_settle(self.sums, piece)

        def sum_relay2(self):
            scatter_relay2(self.sums)

        def give_back(self):
            got = jnp.concatenate(scatter_end(self.sums), axis=0)
            first = half_ep * self.c
            outgoing[first : first + half_ep] = got.reshape(half_ep, cap, COL).astype(BF16)
            send_all(lambda i: return_copy(i, self.c), self.c)
            if self.c == 0:
                returned[ep] = outgoing[own_place]

    near_chunk, far_chunk = Chunk(0), Chunk(1)

    def x_sum_start():
        @pl.when(owner)
        def _():
            whole(st_back, st_enter, 3, slices - 1, 5).wait_recv()

        @pl.when(not_owner)
        def _():
            whole(st_back, st_enter, 3, slices, 5).wait_recv()

        entering = st_enter[...].reshape(COL, COL).astype(BF16)
        head_out = live["local_out"] + lax.dot_general(
            live["q_enter"], entering, (((1,), (1,)), ((), ())), preferred_element_type=F32
        )
        mean = jnp.mean(head_out * head_out, axis=1, keepdims=True)
        gated = head_out * lax.rsqrt(mean + epsilon) * head_gain[...].astype(F32) * live["gate_out"]
        gated = gated.astype(BF16)
        refs = (pxa, pxb, oxa, oxb, nxa, nxb, o2xa, o2xb, n2xa, n2xb)
        live["sums"] = scatters(lambda: gated, wmix, *refs, rsx_s, rsx_r)
        scatter_start(live["sums"])

    def x_sum_relay(piece):
        scatter_relay(live["sums"], piece)

    def x_sum_own():
        scatter_own(live["sums"])

    def x_sum_settle(piece):
        scatter_settle(live["sums"], piece)

    def x_sum_relay2():
        scatter_relay2(live["sums"])

    def x_store():
        got = scatter_end(live["sums"])
        mix_out[0:half_x] = got[0].astype(BF16)
        mix_out[half_x : 2 * half_x] = got[1].astype(BF16)

    def weigh():
        score0, score1 = places[:, 2:3], places[:, 3:4]
        total = score0 + score1
        slot = lax.broadcasted_iota(jnp.int32, (tok, n_ep * cap), 1).astype(F32)
        weight = jnp.where(slot == places[:, 0:1], score0 / total, 0.0)
        weight = weight + jnp.where(slot == places[:, 1:2], score1 / total, 0.0)
        coarse = weight.astype(BF16)
        fine = (weight - coarse.astype(F32)).astype(BF16)
        live.update(coarse=coarse, fine=fine)

    def combine():
        whole(outgoing, returned, 1, half_ep - 1, 2).wait_recv()
        whole(outgoing, returned, 1, half_ep, 3).wait_recv()
        results = returned[...].astype(F32).reshape(n_ep * cap, COL).astype(BF16)
        moe_out[...] = (dot(live["coarse"], results) + dot(live["fine"], results)).astype(BF16)

    send_all(dispatch_copy, 0)
    x_start()
    arrived[own_place] = slots[ep]
    weigh()
    x_near_a()
    send_all(dispatch_copy, 1)
    x_near_b()
    near_chunk.start()
    x_far()
    near_chunk.near()
    x_relays()
    near_chunk.far()
    far_chunk.start()
    x_last()
    near_chunk.relays()
    recurrence()
    far_chunk.near()
    near_chunk.last()
    far_chunk.far()
    near_chunk.experts()
    near_chunk.sum_start()
    far_chunk.relays()
    near_chunk.sum_direct()
    near_chunk.sum_own()
    chain_states()
    far_chunk.last()
    far_chunk.experts()
    far_chunk.sum_start()
    far_chunk.sum_direct()
    far_chunk.sum_relay(0)
    far_chunk.sum_relay(1)
    far_chunk.sum_own()
    near_chunk.sum_relay(0)
    near_chunk.sum_relay(1)
    far_chunk.sum_settle(0)
    far_chunk.sum_settle(1)
    near_chunk.sum_settle(0)
    far_chunk.sum_relay2()
    near_chunk.sum_settle(1)
    x_sum_start()
    far_chunk.give_back()
    near_chunk.sum_relay2()
    x_sum_relay(0)
    x_sum_relay(1)
    near_chunk.give_back()
    x_sum_own()
    x_sum_settle(0)
    x_sum_settle(1)
    x_sum_relay2()
    x_store()
    combine()

    whole(slots, arrived, 0, n_ep - 1).wait_send()
    whole(outgoing, returned, 1, n_ep - 1).wait_send()

    @pl.when(owner)
    def _():
        whole(st_out, st_in, 2, slices - 1).wait_send()
        whole(st_back, st_back, 3, n_ep - 1).wait_send()

    @pl.when(not_owner)
    def _():
        whole(st_out, st_in, 2, slices).wait_send()


def per_device(n_ep, *args):
    (
        mix_rows,
        mix_gain,
        w_query,
        w_forget,
        w_input,
        w_outgate,
        forget_gap,
        decay_extra,
        head_gain,
        w_mixout,
        moe_rows,
        moe_gain,
        route_ids,
        route_scores,
        w_gate,
        w_up,
        w_down,
    ) = args
    tok_a, tok_b = mix_rows.shape[0], moe_rows.shape[0]
    cap = tok_b * route_ids.shape[1] * 3 // (2 * n_ep)
    rows = n_ep * cap
    hidden = w_gate.shape[2]
    width = w_query.shape[0]
    hx, hm = tok_a // 2, rows // 4
    n_tp = SIDE * SIDE
    slices = COL // 8
    hbm = pl.BlockSpec(memory_space=pltpu.HBM)
    dma = pltpu.SemaphoreType.DMA

    def v(shape, dtype=BF16):
        return pltpu.VMEM(shape, dtype)

    def scatter_buffers(h, n=()):
        return [
            v((*n, n_tp, h, COL)),
            v((*n, n_tp, h, COL)),
            v((*n, 2, SIDE, h // 2, COL)),
            v((*n, 2, SIDE, h // 2, COL)),
            v((*n, 2, SIDE, h, COL)),
            v((*n, 2, SIDE, h, COL)),
        ]

    def scatter_ends(h, n=()):
        return [v((*n, 2, h // 2, COL)), v((*n, 2, h // 2, COL)), v((*n, 2, h, COL)), v((*n, 2, h, COL))]

    scratch = [
        v((tok_a, COL)),
        v((tok_b, COL)),
        v((n_tp, COL)),
        v((n_tp, COL)),
        v((1, COL), F32),
        v((1, tok_a), F32),
        v((1, COL)),
        v((2, tok_b), jnp.int32),
        v((2, tok_b), F32),
        v((width, 4 * COL)),
        v((COL, width)),
        v((hidden, width)),
        v((hidden, width)),
        v((hidden, width)),
        v((n_ep, cap, COL)),
        v((n_ep, cap, COL)),
        v((n_ep, cap, COL)),
        v((n_ep, cap, COL)),
        v((tok_b, COL), F32),
        v((2 * n_tp, 1, COL), F32),
        v((n_tp, hx, COL)),
        v((n_tp, hx, COL)),
        v((2, n_tp, hm, COL)),
        v((2, n_tp, hm, COL)),
        v((tok_a, 4 * COL), F32),
        v((tok_a, COL), F32),
        v((rows, hidden), F32),
        v((rows, hidden), F32),
        v((rows, COL), F32),
        v((slices, 16, COL)),
        v((n_ep, 16, COL)),
        v((n_ep, 8, COL), F32),
        v((slices, 8, COL), F32),
        *scatter_buffers(hx),
        *scatter_buffers(hm, (2,)),
        *scatter_ends(hx),
        *scatter_ends(hm, (2,)),
        dma((9,)),
        dma((8,)),
        dma((4,)),
        dma((6,)),
        dma((2,)),
        dma((2, 20)),
        dma((2, 2)),
        dma((2, 2, 20)),
        dma((2,)),
        dma((2, 18)),
        dma((2, 2)),
        dma((2, 2, 18)),
    ]
    return pl.pallas_call(
        functools.partial(step_kernel, n_ep, cap),
        out_shape=[
            v((tok_a, COL)),
            v((tok_b, COL)),
        ],
        in_specs=[hbm] * 17,
        out_specs=[pl.BlockSpec(memory_space=pltpu.VMEM)] * 2,
        scratch_shapes=scratch,
        compiler_params=pltpu.CompilerParams(
            collective_id=0, has_side_effects=True, vmem_limit_bytes=62 * 1024 * 1024
        ),
    )(
        mix_rows,
        moe_rows,
        mix_gain.reshape(-1, COL),
        moe_gain.reshape(-1, COL),
        forget_gap.reshape(1, COL),
        decay_extra,
        head_gain.reshape(1, COL),
        route_ids.T,
        route_scores.T,
        w_query,
        w_forget,
        w_input,
        w_outgate,
        w_mixout,
        jnp.swapaxes(w_gate, 1, 2),
        jnp.swapaxes(w_up, 1, 2),
        w_down,
    )


def solution(mesh):
    placed = (
        P("ep", "tp"),
        P(),
        P(None, "tp"),
        P(None, "tp"),
        P(None, "tp"),
        P(None, "tp"),
        P("tp"),
        P("tp", "ep"),
        P(),
        P("tp", None),
        P("ep", "tp"),
        P(),
        P("ep", None),
        P("ep", None),
        P("ep", None, "tp"),
        P("ep", None, "tp"),
        P("ep", "tp", None),
    )
    return jax.shard_map(
        functools.partial(per_device, mesh.shape["ep"]),
        mesh=mesh,
        in_specs=placed,
        out_specs=(P("ep", "tp"), P("ep", "tp")),
        check_vma=False,
    )
```
